32 devices in a mesh: sp: 8 (over z, y), tp: 4 (over x, core).
Axes of the slice: x: 2, y: 2, z: 4, core: 2. Of those that a mesh axis runs over, the one named last changes fastest.
Arguments:
- queries: bfloat16 [1024, 2048], P('sp', 'tp'), may hold values from -6 to 6
- keys: bfloat16 [1024, 512], P('sp', 'tp'), may hold values from -6 to 6
- values: bfloat16 [1024, 512], P('sp', 'tp'), may hold values from -6 to 6
- query_gain: float32 [128], replicated, may hold values from 0.3 to 7
- key_norm_gain: float32 [128], replicated, may hold values from 0.3 to 7
- out_weight: bfloat16 [2048, 2048], P('tp'), may hold values from -0.25 to 0.25
- residual: bfloat16 [1024, 2048], P(('sp', 'tp')), may hold values from -6 to 6
- norm_gain: float32 [2048], replicated, may hold values from 0.1 to 1.9
- expert_gate: bfloat16 [8, 2048, 3072], P('sp', None, 'tp'), may hold values from -0.125 to 0.125
- expert_up: bfloat16 [8, 2048, 3072], P('sp', None, 'tp'), may hold values from -0.125 to 0.125
- expert_down: bfloat16 [8, 3072, 2048], P('sp', 'tp'), may hold values from -0.109375 to 0.109375
- routes: int32 [1024, 2], P(('sp', 'tp')), may hold values from 0 to 7, all different within a row; in each aligned block of 32 rows (0 to 31, 32 to 63, ...) at most 16 rows name the same one
- route_weight: float32 [1024, 2], P(('sp', 'tp')), may hold values from 0.25 to 1
Outputs:
- mixed: bfloat16 [1024, 2048], P(('sp', 'tp'))
The draws below stay inside these ranges and needn't reach their ends.
Inputs may be any that keep to these rules, and one draw needn't show every extreme that they name: The two experts of a token differ. In each aligned block of 32 tokens (the tokens of one device), no expert is named by more than 16 routes, and in some block one expert is named by exactly 16.
All inputs are finite; a program needn't handle non-finite values.
Results may differ from the reference program's by a relative error of at most 0.013.
The reference program's roundings to bfloat16 on the way count: a program that leaves them out, or rounds other values in their place, can miss the bound.
Values may be sent and summed in bfloat16 or wider, within the bound.
A program may use at most 64 MiB of HBM per device.

```python
import math
import jax
import jax.numpy as jnp
import numpy as np
from jax import lax

D = 2048
QUERY_HEAD_COUNT = 16
KEY_VALUE_HEADS = 4
HEAD_SIZE = 128
FE = 3072
TOP = 2
GRID_W = 64
TOK_DEV = 128
SEQUENCE_TOKENS = 1024
EXPERTS = 8
CAP = 16
N_SP = 8
N_TP = 4


def shared_gain(key, salt_value):
    uniform_unit = jax.random.uniform(jax.random.fold_in(key, salt_value), (HEAD_SIZE,), jnp.float32)
    return jnp.exp(jnp.log(1.2) + uniform_unit * (jnp.log(2.5) - jnp.log(1.2)))


def draw_query_gain(key, part):
    return shared_gain(key, 102)


def draw_key_norm_gain(key, part):
    return shared_gain(key, 103)


def build_keys(key):
    base_sample = jnp.clip(jax.random.normal(jax.random.fold_in(key, 104), (SEQUENCE_TOKENS, KEY_VALUE_HEADS * HEAD_SIZE), jnp.float32), -6.0, 6.0)
    return base_sample


def draw_keys(key, part):
    return build_keys(key).astype(jnp.bfloat16)


def draw_queries(key, part):
    base_sample = jnp.clip(jax.random.normal(jax.random.fold_in(key, 105), (SEQUENCE_TOKENS, QUERY_HEAD_COUNT * HEAD_SIZE), jnp.float32), -6.0, 6.0)
    return base_sample.astype(jnp.bfloat16)


def levels(stream_key, dims, cuts, smallest, top_value):
    def one(position, shards_of):
        steps = jax.random.uniform(jax.random.fold_in(jax.random.fold_in(stream_key, 6), position), (shards_of,), jnp.float32, smallest / len(cuts), top_value / len(cuts))
        return jnp.repeat(jnp.exp(steps), dims[position] // shards_of).reshape((-1,) + (1,) * (len(dims) - position - 1))

    level = one(*cuts[0])
    for cut in cuts[1:]:
        level = level * one(*cut)
    return level


def assign_block(key, own, number, rows, amount, top, reach, skew):
    ranking = jax.random.permutation(key, amount)
    crowded, usual = portions_of(amount, rows * top, reach, skew, True), portions_of(amount, rows * top, reach, skew, False)
    places = jnp.arange(amount)

    def named(sizes, rotation):
        used = int((sizes > 0).sum())
        fixed = max(1, used // 4)
        shifted = fixed + (places - fixed + rotation * (used - fixed)) % max(1, amount - fixed)
        return jnp.zeros((amount,), jnp.int32).at[ranking[jnp.where(places < fixed, places, shifted)]].set(jnp.asarray(sizes, jnp.int32))

    sizes = jnp.where(number % 4 == 0, named(crowded, number // 4), named(usual, number - number // 4 - 1))
    mixed = jax.random.permutation(jax.random.fold_in(own, 3), amount)
    donor, sink = mixed[0:amount // 2 * 2:2], mixed[1:amount // 2 * 2:2]
    margin = jnp.minimum(sizes[donor] - 1, reach - sizes[sink]) // 2
    margin = jnp.where((donor == ranking[0]) | (sink == ranking[0]) | (sizes[sink] == 0), 0, jnp.maximum(margin, 0))
    shifted = jax.random.randint(jax.random.fold_in(own, 4), (amount // 2,), 0, 1 << 20) % (margin + 1)
    sizes = sizes.at[donor].add(-shifted).at[sink].add(shifted)
    labels = jnp.searchsorted(jnp.cumsum(sizes), jnp.arange(rows * top), side="right").astype(jnp.int32)
    grid = labels.reshape(top, rows).T
    grid = grid[jax.random.permutation(jax.random.fold_in(own, 1), rows)]
    rotation = jax.random.randint(jax.random.fold_in(own, 2), (rows, 1), 0, top)
    return jnp.take_along_axis(grid, (jnp.arange(top)[None, :] + rotation) % top, axis=1)


def portions_of(count, total, bound, skew, full):
    portions = [(1 << 20) // math.isqrt(standing ** skew) + 1 for standing in range(1, count + 1)]
    largest = bound if full else min(bound, max(-(-total // count), total * portions[0] // sum(portions)))
    least = 1 if total - largest >= count - 1 else 0
    holding, spare = [largest] + [least] * (count - 1), total - largest - least * (count - 1)
    while spare > 0:
        free = [i for i in range(1, count) if holding[i] < largest] or [i for i in range(1, count) if holding[i] < bound]
        whole, budget = sum([portions[i] for i in free]), spare
        for i in free:
            extra = min(bound - holding[i], max(1, budget * portions[i] // whole), spare)
            holding[i] = holding[i] + extra
            spare = spare - extra
    return np.array(holding)


def bell_draw(rng, shape, width, reach, split=(), kind=jnp.bfloat16):
    entries = jax.random.normal(rng, shape, jnp.float32) * width
    if len(split) > 0:
        entries = levels(rng, shape, split, -0.22, 0.18) * entries
    return jnp.clip(entries, min=-reach, max=reach).astype(kind)


def setup_inputs(seed: int = 0) -> dict:
    streams_of = jax.random.split(jax.random.key(seed), 14)
    queries = draw_queries(jax.random.fold_in(streams_of[13], 71), 0)
    keys = draw_keys(jax.random.fold_in(streams_of[13], 71), 0)
    values = bell_draw(streams_of[2], (SEQUENCE_TOKENS, KEY_VALUE_HEADS * HEAD_SIZE), 1.0, 6.0, ((0, 8), (1, 4)))
    query_gain = draw_query_gain(jax.random.fold_in(streams_of[13], 71), 0)
    key_norm_gain = draw_key_norm_gain(jax.random.fold_in(streams_of[13], 71), 0)
    out_weight = bell_draw(streams_of[5], (QUERY_HEAD_COUNT * HEAD_SIZE, D), (QUERY_HEAD_COUNT * HEAD_SIZE // 4) ** -0.5, 0.25, ((0, 4),))
    residual = bell_draw(streams_of[6], (SEQUENCE_TOKENS, D), 1.0, 6.0, ((0, 32),))
    norm_gain = jnp.clip(1.0 + 0.18 * jax.random.normal(streams_of[7], (D,), jnp.float32), 0.1, 1.9)
    expert_gate = bell_draw(streams_of[8], (EXPERTS, D, FE), D ** -0.5, 0.125, ((0, 8), (2, 4)))
    expert_up = bell_draw(streams_of[9], (EXPERTS, D, FE), D ** -0.5, 0.125, ((0, 8), (2, 4)))
    expert_down = bell_draw(streams_of[10], (EXPERTS, FE, D), FE ** -0.5, 0.109375, ((0, 8), (1, 4)))
    routes_keys = jax.random.split(jax.random.fold_in(streams_of[11], 1), SEQUENCE_TOKENS // (TOK_DEV // N_TP))
    routes_turns = jax.random.permutation(jax.random.fold_in(streams_of[11], 3), SEQUENCE_TOKENS // (TOK_DEV // N_TP))
    routes = jax.vmap(lambda own, number: assign_block(jax.random.fold_in(streams_of[11], 2), own, number, TOK_DEV // N_TP, EXPERTS, TOP, CAP, 2))(routes_keys, routes_turns).reshape((SEQUENCE_TOKENS, TOP))
    route_weight = jnp.clip(0.25 + 0.75 * jax.random.uniform(streams_of[12], (SEQUENCE_TOKENS, TOP), jnp.float32) ** levels(streams_of[12], (SEQUENCE_TOKENS, TOP), ((0, 32),), -0.2, 0.2), 0.25, 1.0)
    return {"queries": queries, "keys": keys, "values": values, "query_gain": query_gain, "key_norm_gain": key_norm_gain, "out_weight": out_weight, "residual": residual, "norm_gain": norm_gain, "expert_gate": expert_gate, "expert_up": expert_up, "expert_down": expert_down, "routes": routes, "route_weight": route_weight}


norm_eps = 1e-06
theta_base = 10000.0

def round_to_half(array):
    return lax.optimization_barrier(array.astype(jnp.bfloat16)).astype(jnp.float32)

def head_normalize(packed, gain, heads):
    heads_float = packed.astype(jnp.float32).reshape(packed.shape[0], heads, HEAD_SIZE)
    scaled = heads_float * lax.rsqrt(lax.optimization_barrier(jnp.mean(heads_float * heads_float, axis=-1, keepdims=True)) + norm_eps)
    return scaled * gain.astype(jnp.float32)

def rotary_tables(positions):
    freq_count = HEAD_SIZE // 4
    grid_row = (positions // GRID_W).astype(jnp.float32)
    grid_col = (positions % GRID_W).astype(jnp.float32)
    inverse = theta_base ** (-jnp.arange(freq_count, dtype=jnp.float32) * 2.0 / (HEAD_SIZE // 2))
    by_row = grid_row[:, None] * inverse
    by_col = grid_col[:, None] * inverse
    angles = jnp.concatenate([by_row, by_row, by_col, by_col], axis=-1)
    return (jnp.cos(angles), jnp.sin(angles))

def apply_rotation(heads_float, cosine_table, sine_values):
    freq_count = HEAD_SIZE // 4
    split_head = heads_float.reshape(heads_float.shape[:-1] + (2, 2, freq_count))
    turned = jnp.stack([-split_head[..., 1, :], split_head[..., 0, :]], axis=-2).reshape(heads_float.shape)
    return heads_float * cosine_table[:, None, :] + turned * sine_values[:, None, :]

def reference(queries, keys, values, query_gain, key_norm_gain, out_weight, residual, norm_gain, expert_gate, expert_up, expert_down, routes, route_weight):
    score_scale = 1.0 / math.sqrt(HEAD_SIZE)
    group_members = QUERY_HEAD_COUNT // KEY_VALUE_HEADS
    positions = jnp.arange(SEQUENCE_TOKENS, dtype=jnp.int32)
    cosine_table, sine_values = rotary_tables(positions)
    rotated_queries = apply_rotation(head_normalize(queries, query_gain, QUERY_HEAD_COUNT), cosine_table, sine_values).astype(jnp.bfloat16)
    rotated_keys = round_to_half(apply_rotation(head_normalize(keys, key_norm_gain, KEY_VALUE_HEADS), cosine_table, sine_values))
    value_wide_float = values.reshape(SEQUENCE_TOKENS, KEY_VALUE_HEADS, HEAD_SIZE).astype(jnp.float32)
    query_tile_rows = math.gcd(SEQUENCE_TOKENS, 128)
    block_list = rotated_queries.reshape(SEQUENCE_TOKENS // query_tile_rows, query_tile_rows, KEY_VALUE_HEADS, group_members, HEAD_SIZE)

    def attend(query_part):
        scores = jnp.einsum('qkgd,skd->kgqs', query_part.astype(jnp.float32), rotated_keys) * score_scale
        row_max = lax.optimization_barrier(jnp.max(scores, axis=-1, keepdims=True))
        weights = jnp.exp(scores - row_max)
        norm_sum = lax.optimization_barrier(jnp.sum(weights, axis=-1))
        value_sum = jnp.einsum('kgqs,skd->kgqd', round_to_half(weights), value_wide_float)
        result = value_sum / norm_sum[..., None]
        return result.transpose(2, 0, 1, 3).reshape(query_tile_rows, QUERY_HEAD_COUNT * HEAD_SIZE).astype(jnp.bfloat16)
    attention = lax.map(attend, block_list).reshape(SEQUENCE_TOKENS, QUERY_HEAD_COUNT * HEAD_SIZE)
    projected = jnp.dot(attention, out_weight, preferred_element_type=jnp.float32)
    hidden_state = residual.astype(jnp.float32) + projected
    normed = (hidden_state * lax.rsqrt(lax.optimization_barrier(jnp.mean(hidden_state * hidden_state, axis=-1, keepdims=True)) + norm_eps) * norm_gain.astype(jnp.float32)).astype(jnp.bfloat16)
    slots_most = N_SP * N_TP * CAP
    flat_routes = routes.reshape(-1)
    flat_weight = route_weight.reshape(-1).astype(jnp.float32)
    piece_width = FE // N_TP

    def expert_step(total, inputs):
        expert, gate_weight, up_weight, down_weight = inputs
        chosen = flat_routes == expert
        route_index = jnp.nonzero(chosen, size=slots_most, fill_value=0)[0].astype(jnp.int32)
        live_mask = (jnp.arange(slots_most, dtype=jnp.int32) < jnp.sum(chosen.astype(jnp.int32))).astype(jnp.float32)
        owner_row = route_index // TOP
        rows_in = normed[owner_row]
        gate_proj = jnp.dot(rows_in, gate_weight, preferred_element_type=jnp.float32)
        up_proj = jnp.dot(rows_in, up_weight, preferred_element_type=jnp.float32)
        hidden_act = (jax.nn.silu(gate_proj) * up_proj).astype(jnp.bfloat16)
        summed = jnp.zeros((slots_most, D), jnp.float32)
        for quarter in range(N_TP):
            down_part = jnp.dot(hidden_act[:, quarter * piece_width:(quarter + 1) * piece_width], down_weight[quarter * piece_width:(quarter + 1) * piece_width], preferred_element_type=jnp.float32)
            summed = summed + round_to_half(down_part)
        output = round_to_half(summed)
        total = total.at[owner_row].add((flat_weight[route_index] * live_mask)[:, None] * output)
        return (total, None)
    moe_sum, _ = lax.scan(expert_step, jnp.zeros((SEQUENCE_TOKENS, D), jnp.float32), (jnp.arange(EXPERTS, dtype=jnp.int32), expert_gate, expert_up, expert_down))
    return (hidden_state + moe_sum).astype(jnp.bfloat16)
```

```python
import functools
import math

import jax
import jax.numpy as jnp
import numpy as np
from jax import lax
from jax.experimental import pallas as pl
from jax.experimental.pallas import tpu as pltpu
from jax.sharding import PartitionSpec as P

HEAD_SIZE = 128
GRID_W = 64


norm_eps = 1e-06
theta_base = 10000.0


def head_normalize(packed, gain, heads):
    heads_float = packed.astype(jnp.float32).reshape(packed.shape[0], heads, HEAD_SIZE)
    scaled = heads_float * lax.rsqrt(
        jnp.mean(heads_float * heads_float, axis=-1, keepdims=True) + norm_eps
    )
    return scaled * gain


def rotary_tables(positions):
    freq_count = HEAD_SIZE // 4
    grid_row = (positions // GRID_W).astype(jnp.float32)
    grid_col = (positions % GRID_W).astype(jnp.float32)
    inverse = theta_base ** (-jnp.arange(freq_count, dtype=jnp.float32) * 2.0 / (HEAD_SIZE // 2))
    by_row = grid_row[:, None] * inverse
    by_col = grid_col[:, None] * inverse
    angles = jnp.concatenate([by_row, by_row, by_col, by_col], axis=-1)
    return (jnp.cos(angles), jnp.sin(angles))


def apply_rotation(heads_float, cosine_table, sine_values):
    freq_count = HEAD_SIZE // 4
    split_head = heads_float.reshape(heads_float.shape[:-1] + (2, 2, freq_count))
    turned = jnp.stack([-split_head[..., 1, :], split_head[..., 0, :]], axis=-2).reshape(
        heads_float.shape
    )
    return heads_float * cosine_table[:, None, :] + turned * sine_values[:, None, :]


def on_device(
    queries,
    keys,
    values,
    query_gain,
    key_norm_gain,
    out_weight,
    residual,
    norm_gain,
    expert_gate,
    expert_up,
    expert_down,
    routes,
    route_weight,
):
    local_rows = queries.shape[0]
    query_heads = queries.shape[1] // HEAD_SIZE
    key_heads = keys.shape[1] // HEAD_SIZE
    group_members = query_heads // key_heads
    score_scale = 1.0 / math.sqrt(HEAD_SIZE)
    positions = lax.axis_index("sp") * local_rows + jnp.arange(local_rows, dtype=jnp.int32)
    cosine_table, sine_values = rotary_tables(positions)
    rotated_queries = apply_rotation(
        head_normalize(queries, query_gain, query_heads), cosine_table, sine_values
    ).astype(jnp.bfloat16)
    query_block = rotated_queries.reshape(
        local_rows, key_heads, group_members, HEAD_SIZE
    ).transpose(1, 2, 0, 3)
    query_block = query_block.reshape(key_heads, group_members * local_rows, HEAD_SIZE)
    rotated_keys = apply_rotation(
        head_normalize(keys, key_norm_gain, key_heads), cosine_table, sine_values
    ).astype(jnp.bfloat16)
    rotated_keys = rotated_keys.reshape(local_rows, key_heads * HEAD_SIZE)
    start_state = (
        jnp.full((key_heads, group_members * local_rows), -1e30, jnp.float32),
        jnp.zeros((key_heads, group_members * local_rows), jnp.float32),
        jnp.zeros((key_heads, group_members * local_rows, HEAD_SIZE), jnp.float32),
    )
    folded = start_state
    key_piece = lax.all_gather(rotated_keys, "sp", axis=0, tiled=True)
    value_piece = lax.all_gather(values, "sp", axis=0, tiled=True)
    key_count = key_piece.shape[0]
    span_size = 512
    key_spans = key_piece.reshape(key_count // span_size, span_size, key_heads, HEAD_SIZE)
    value_spans = value_piece.reshape(key_count // span_size, span_size, key_heads, HEAD_SIZE)

    def one_span(state, span_pair):
        running, norm_sum, gathered_sum = state
        key_span, value_span = span_pair
        scores = (
            jnp.einsum("hqd,khd->hqk", query_block, key_span, preferred_element_type=jnp.float32)
            * score_scale
        )
        newest = jnp.maximum(running, jnp.max(scores, axis=-1))
        shrink = jnp.exp(running - newest)
        weights = jnp.exp(scores - newest[..., None])
        norm_sum = norm_sum * shrink + jnp.sum(weights, axis=-1)
        gathered_sum = gathered_sum * shrink[..., None] + jnp.einsum(
            "hqk,khd->hqd",
            weights.astype(jnp.bfloat16),
            value_span,
            preferred_element_type=jnp.float32,
        )
        return ((newest, norm_sum, gathered_sum), None)

    folded, _ = lax.scan(one_span, folded, (key_spans, value_spans))
    running, norm_sum, gathered_sum = folded
    attention = (gathered_sum / norm_sum[..., None]).reshape(
        key_heads, group_members, local_rows, HEAD_SIZE
    )
    attention = (
        attention.transpose(2, 0, 1, 3)
        .reshape(local_rows, query_heads * HEAD_SIZE)
        .astype(jnp.bfloat16)
    )
    out_rows = residual.shape[0]
    model_width = residual.shape[1]
    projected = lax.psum_scatter(
        jnp.dot(attention, out_weight, preferred_element_type=jnp.float32).astype(jnp.bfloat16),
        "tp",
        scatter_dimension=0,
        tiled=True,
    ).astype(jnp.float32)
    hidden_state = residual.astype(jnp.float32) + projected
    normed = (
        hidden_state
        * lax.rsqrt(jnp.mean(hidden_state * hidden_state, axis=-1, keepdims=True) + norm_eps)
        * norm_gain
    ).astype(jnp.bfloat16)
    route_top = routes.shape[1]
    group_width = lax.axis_size("tp")
    expert_count = lax.axis_size("sp") * expert_gate.shape[0]
    capacity = 2 * max(1, route_top * local_rows // (group_width * expert_count))
    flat_routes = routes.reshape(-1)
    onehot = (flat_routes[:, None] == jnp.arange(expert_count, dtype=jnp.int32)[None, :]).astype(
        jnp.int32
    )
    earlier = jnp.cumsum(onehot, axis=0) - onehot
    slot_rank = jnp.sum(earlier * onehot, axis=1)
    slot_index = flat_routes * capacity + slot_rank
    placer = (
        jnp.arange(expert_count * capacity, dtype=jnp.int32)[:, None] == slot_index[None, :]
    ).astype(jnp.bfloat16)
    route_rows = jnp.repeat(normed, route_top, axis=0)
    buffer = jnp.dot(placer, route_rows, preferred_element_type=jnp.float32).astype(jnp.bfloat16)
    buffer = buffer.reshape(expert_count, capacity, model_width)
    mail_rows = lax.all_to_all(buffer, "sp", split_axis=0, concat_axis=0, tiled=True)
    inbox_rows = lax.all_gather(mail_rows, "tp", axis=1, tiled=True)
    source_count = inbox_rows.shape[0]
    rows_in = inbox_rows.reshape(-1, model_width)
    gate_proj = jnp.dot(rows_in, expert_gate[0], preferred_element_type=jnp.float32)
    up_proj = jnp.dot(rows_in, expert_up[0], preferred_element_type=jnp.float32)
    hidden_act = (jax.nn.silu(gate_proj) * up_proj).astype(jnp.bfloat16)
    down_part = jnp.dot(hidden_act, expert_down[0], preferred_element_type=jnp.float32)
    down_part = down_part.reshape(source_count, group_width * capacity, model_width)
    summed = lax.psum_scatter(down_part.astype(jnp.bfloat16), "tp", scatter_dimension=1, tiled=True)
    returned = lax.all_to_all(summed, "sp", split_axis=0, concat_axis=0, tiled=True)
    per_route = jnp.dot(
        placer.T, returned.reshape(-1, model_width), preferred_element_type=jnp.float32
    )
    per_route = per_route.reshape(out_rows, route_top, model_width)
    moe_sum = jnp.sum(route_weight[:, :, None] * per_route, axis=1)
    return (hidden_state + moe_sum).astype(jnp.bfloat16)


MESH = pl.DeviceIdType.MESH
LOG2E = 1.4426950408889634


def layer_kernel(
    dims,
    row_hbm,
    column_hbm,
    k_hbm,
    kgain_hbm,
    v_hbm,
    q_hbm,
    qgain_hbm,
    wout_hbm,
    routes_hbm,
    weight_hbm,
    resid_hbm,
    ngain_hbm,
    gate_hbm,
    up_hbm,
    down_hbm,
    out_ref,
    row_ref,
    column_ref,
    k_ref,
    kgain_ref,
    v_ref,
    q_ref,
    qgain_ref,
    routes_ref,
    weight_ref,
    resid_ref,
    ngain_ref,
    picks,
    placed_ref,
    wcol,
    wout,
    wgate,
    wup,
    wdown,
    kv,
    att,
    part,
    rs_in,
    state,
    mail,
    inbox,
    hidden,
    keep,
    pair_out,
    pair_in,
    xsum,
    xin,
    outmail,
    back,
    wsem,
    kv_send,
    kv_fsend,
    kv_recv,
    rs_send,
    rs_recv,
    mail_send,
    x_send,
    p_send,
    f_send,
    in_recv,
    pair_send,
    pair_recv,
    rx_send,
    rx_recv,
    back_send,
    back_recv,
):
    nsp, ntp, heads, cap, rows, own_rows = dims
    width = out_ref.shape[1]
    span = nsp // 2
    me = lax.axis_index("sp")
    tp = lax.axis_index("tp")
    far = me // 2
    near = me % 2
    side = tp // 2
    core = tp % 2
    mate = side * 2 + (1 - core)
    across = (1 - side) * 2 + core
    diagonal = (1 - side) * 2 + (1 - core)
    twin = far * 2 + (1 - near)

    def flip(index, mask):
        value, bit = 0, 1
        while bit < nsp:
            digit = (index // bit) % 2
            value = value + bit * (1 - digit if mask & bit else digit)
            bit *= 2
        return value

    def peer(d):
        return flip(me, d)

    loads = []
    for i, (hbm, local) in enumerate(
        (
            (k_hbm, k_ref),
            (kgain_hbm, kgain_ref),
            (row_hbm.at[me], row_ref),
            (column_hbm, column_ref),
            (v_hbm, kv.at[me, :, pl.ds(HEAD_SIZE, HEAD_SIZE)]),
            (q_hbm, q_ref),
            (qgain_hbm, qgain_ref),
            (routes_hbm, routes_ref),
            (weight_hbm, weight_ref),
            (resid_hbm, resid_ref),
            (ngain_hbm, ngain_ref),
            (wout_hbm, wout),
            (gate_hbm.at[0], wgate),
            (up_hbm.at[0], wup),
            (down_hbm.at[0], wdown),
        )
    ):
        load = pltpu.make_async_copy(hbm, local, wsem.at[i])
        load.start()
        loads.append(load)

    barrier = pltpu.get_barrier_semaphore()
    for d in range(1, nsp):
        pl.semaphore_signal(barrier, inc=1, device_id=(peer(d), tp), device_id_type=MESH)
    for d in range(1, ntp):
        pl.semaphore_signal(
            barrier, inc=1, device_id=(me, lax.rem(tp + d, ntp)), device_id_type=MESH
        )

    sent = []

    def push(source, target, send_sem, recv_sem, to_sp, to_tp):
        copy = pltpu.make_async_remote_copy(
            src_ref=source,
            dst_ref=target,
            send_sem=send_sem,
            recv_sem=recv_sem,
            device_id=(to_sp, to_tp),
            device_id_type=MESH,
        )
        copy.start()
        sent.append(copy)

    def arrived(target, send_sem, recv_sem):
        pltpu.make_async_remote_copy(
            src_ref=target,
            dst_ref=target,
            send_sem=send_sem,
            recv_sem=recv_sem,
            device_id=(twin, tp),
            device_id_type=MESH,
        ).wait_recv()

    lane = lax.broadcasted_iota(jnp.int32, (1, HEAD_SIZE), 1)
    leading = lane % (HEAD_SIZE // 2) < HEAD_SIZE // 4

    def table(part):
        lanes = slice(part * HEAD_SIZE, (part + 1) * HEAD_SIZE)
        by_column = column_ref[:, lanes]
        return jnp.concatenate(
            [
                jnp.where(lane < HEAD_SIZE // 2, row_ref[k : k + 1, lanes], by_column)
                for k in range(row_ref.shape[0])
            ],
            axis=0,
        )

    def turned(head, gain_ref, tables):
        cosine, sine_a, sine_b = tables
        wide = head.astype(jnp.float32)
        scaled = wide * lax.rsqrt(jnp.mean(wide * wide, axis=-1, keepdims=True) + norm_eps)
        scaled = scaled * gain_ref[...]
        quarter = HEAD_SIZE // 4
        return (
            scaled * cosine
            + pltpu.roll(scaled, HEAD_SIZE - quarter, 1) * sine_a
            + pltpu.roll(scaled, quarter, 1) * sine_b
        ).astype(jnp.bfloat16)

    for i in (0, 1, 2, 3):
        loads[i].wait()
    sine = table(1)
    tables = (table(0), jnp.where(leading, -sine, 0.0), jnp.where(leading, 0.0, sine))
    kv[me, :, :HEAD_SIZE] = turned(k_ref[...], kgain_ref, tables)
    loads[4].wait()
    pl.semaphore_wait(barrier, nsp - 1 + ntp - 1)

    push(kv.at[me], kv.at[me], kv_send.at[0], kv_recv.at[me], twin, tp)
    for d in range(1, span):
        push(kv.at[me], kv.at[me], kv_send.at[d], kv_recv.at[me], peer(2 * d), tp)

    loads[5].wait()
    loads[6].wait()
    queries = [
        turned(q_ref[:, h * HEAD_SIZE : (h + 1) * HEAD_SIZE], qgain_ref, tables)
        for h in range(heads)
    ]
    for h in range(heads):
        att[:, h * HEAD_SIZE : (h + 1) * HEAD_SIZE] = queries[h]

    loads[7].wait()
    loads[8].wait()
    which = lax.broadcasted_iota(jnp.int32, (nsp, own_rows), 0)
    named = [which == routes_ref[j : j + 1, :] for j in range(routes_ref.shape[0])]
    named = [jnp.where(hit, 1.0, 0.0) for hit in named]
    hits = functools.reduce(jnp.add, named)
    square = (own_rows, own_rows)
    one, two = (lax.broadcasted_iota(jnp.int32, square, axis) for axis in (0, 1))
    rank = jnp.dot(
        hits.astype(jnp.bfloat16),
        jnp.where(one < two, 1.0, 0.0).astype(jnp.bfloat16),
        preferred_element_type=jnp.float32,
    )
    places = lax.broadcasted_iota(jnp.int32, (nsp, cap, own_rows), 1)
    ranked = jnp.where(places == rank.astype(jnp.int32)[:, None, :], 1.0, 0.0)
    placer = (ranked * hits[:, None, :]).reshape(nsp * cap, own_rows).astype(jnp.bfloat16)
    for j, hit in enumerate(named):
        picks[j] = (ranked * hit[:, None, :]).reshape(nsp * cap, own_rows).astype(jnp.bfloat16)
        column = jnp.sum(
            jnp.where(one == two, weight_ref[j : j + 1, :], 0.0), axis=1, keepdims=True
        )
        wcol[j] = jnp.broadcast_to(column, wcol.shape[1:])
    placed_ref[...] = placer

    for d in range(1, span):
        source = peer(2 * d)
        arrived(kv.at[source], kv_send.at[0], kv_recv.at[source])
        push(kv.at[source], kv.at[source], kv_fsend.at[d], kv_recv.at[source], twin, tp)
    for d in range(span):
        source = peer(2 * d + 1)
        arrived(kv.at[source], kv_send.at[0], kv_recv.at[source])

    scale = LOG2E / math.sqrt(HEAD_SIZE)
    for h in range(heads):
        columns = slice(h * HEAD_SIZE, (h + 1) * HEAD_SIZE)
        all_keys = kv[:, :, :HEAD_SIZE].reshape(nsp * rows, HEAD_SIZE)
        scores = lax.dot_general(
            att[:, columns],
            all_keys,
            (((1,), (1,)), ((), ())),
            preferred_element_type=jnp.float32,
        )
        top = jnp.max(scores, axis=-1, keepdims=True)
        weights = jnp.exp2((scores - top) * scale)
        norm_sum = jnp.sum(weights, axis=-1, keepdims=True)
        all_values = kv[:, :, HEAD_SIZE:].reshape(nsp * rows, HEAD_SIZE)
        mixed = jnp.dot(
            weights.astype(jnp.bfloat16), all_values, preferred_element_type=jnp.float32
        )
        att[:, columns] = (mixed / norm_sum).astype(jnp.bfloat16)

    loads[11].wait()
    tile = 512

    @pl.loop(0, width // tile)
    def _(j):
        columns = pl.ds(pl.multiple_of(j * tile, tile), tile)
        product = jnp.dot(att[...], wout[:, columns], preferred_element_type=jnp.float32)
        part[:, :, columns] = product.astype(jnp.bfloat16).reshape(ntp, own_rows, tile)

    push(part.at[diagonal], rs_in.at[1], rs_send.at[1], rs_recv.at[1], me, mate)
    push(part.at[mate], rs_in.at[2], rs_send.at[2], rs_recv.at[2], me, mate)
    arrived(rs_in.at[1], rs_send.at[1], rs_recv.at[1])
    part[across] = (
        part[across].astype(jnp.float32) + rs_in[1].astype(jnp.float32)
    ).astype(jnp.bfloat16)
    push(part.at[across], rs_in.at[3], rs_send.at[3], rs_recv.at[3], me, across)
    loads[9].wait()
    loads[10].wait()
    total = resid_ref[...].astype(jnp.float32) + part[tp].astype(jnp.float32)
    for d in (2, 3):
        arrived(rs_in.at[d], rs_send.at[d], rs_recv.at[d])
        total = total + rs_in[d].astype(jnp.float32)
    state[...] = total
    normed = (
        total
        * lax.rsqrt(jnp.mean(total * total, axis=-1, keepdims=True) + norm_eps)
        * ngain_ref[...]
    ).astype(jnp.bfloat16)
    mail[...] = (
        jnp.dot(placed_ref[...], normed, preferred_element_type=jnp.float32)
        .astype(jnp.bfloat16)
        .reshape(nsp, cap, width)
    )
    half = nsp // 2
    quarter = nsp // 4
    first = [*range(quarter), *range(half, half + quarter)]
    groups = (first, [d for d in range(nsp) if d not in first])
    relay = groups[0] + groups[1]
    leaving = sorted(first, reverse=True) + sorted(groups[1], reverse=True)
    for d in leaving:
        if d:
            to = peer(d)
            push(mail.at[to], inbox.at[tp, me], mail_send.at[d], in_recv.at[tp, me], to, tp)
    inbox[tp, me] = mail[me]

    def wait_piece(owner, d):
        source = peer(d)
        arrived(inbox.at[owner, source], mail_send.at[0], in_recv.at[owner, source])

    def spread(g):
        for d in groups[g]:
            if d:
                wait_piece(tp, d)
            piece = inbox.at[tp, peer(d)]
            arrival = in_recv.at[tp, peer(d)]
            push(piece, piece, x_send.at[d], arrival, me, across)
            push(piece, piece, p_send.at[d], arrival, me, mate)

    def forward(g):
        for d in groups[g]:
            wait_piece(across, d)
            piece = inbox.at[across, peer(d)]
            arrival = in_recv.at[across, peer(d)]
            push(piece, piece, f_send.at[d], arrival, me, mate)
        for d in groups[g]:
            wait_piece(diagonal, d)

    fine = 256

    def experts(parts):
        blocks = [(owner, peer(d)) for owner, _, g in parts for d in groups[g]]
        live = len(blocks) * cap

        @pl.loop(0, wgate.shape[1] // fine)
        def _(j):
            columns = pl.ds(pl.multiple_of(j * fine, fine), fine)
            block = jnp.concatenate([inbox[owner, source] for owner, source in blocks], axis=0)
            gate = jnp.dot(block, wgate[:, columns], preferred_element_type=jnp.float32)
            up = jnp.dot(block, wup[:, columns], preferred_element_type=jnp.float32)
            hidden[:live, columns] = (gate / (1.0 + jnp.exp(-gate)) * up).astype(jnp.bfloat16)

        @pl.loop(0, width // tile)
        def _(j):
            columns = pl.ds(pl.multiple_of(j * tile, tile), tile)
            product = jnp.dot(hidden[:live], wdown[:, columns], preferred_element_type=jnp.float32)
            product = product.reshape(len(parts), half, cap, tile)
            for i, (_, target, g) in enumerate(parts):
                target[g * half : (g + 1) * half, :, columns] = product[i].astype(target.dtype)

    def hand(i, g):
        span_of = pl.ds(g * half, half)
        k = 2 * i + g
        push(
            pair_out.at[i, span_of],
            pair_in.at[i, span_of],
            pair_send.at[k],
            pair_recv.at[k],
            me,
            mate,
        )

    def take(i, g):
        span_of = pl.ds(g * half, half)
        k = 2 * i + g
        arrived(pair_in.at[i, span_of], pair_send.at[k], pair_recv.at[k])

    def cross(g):
        take(1, g)
        for d in sorted(groups[g], reverse=True):
            slot = g * half + groups[g].index(d)
            source = peer(d)
            xsum[source] = (keep[1, slot] + pair_in[1, slot].astype(jnp.float32)).astype(
                jnp.bfloat16
            )
            push(
                xsum.at[source], xin.at[source], rx_send.at[d], rx_recv.at[source], me, across
            )

    spread(0)
    for i in (12, 13, 14):
        loads[i].wait()
    for d in groups[0]:
        wait_piece(mate, d)
    experts([(tp, keep.at[0], 0), (mate, pair_out.at[0], 0)])
    hand(0, 0)
    spread(1)
    forward(0)
    experts([(diagonal, pair_out.at[1], 0), (across, keep.at[1], 0)])
    hand(1, 0)
    cross(0)
    for d in groups[1]:
        wait_piece(mate, d)
    forward(1)
    experts(
        [
            (diagonal, pair_out.at[1], 1),
            (across, keep.at[1], 1),
            (tp, keep.at[0], 1),
            (mate, pair_out.at[0], 1),
        ]
    )
    hand(1, 1)
    hand(0, 1)
    cross(1)
    for d in leaving:
        g = 0 if d in first else 1
        slot = g * half + groups[g].index(d)
        source = peer(d)
        if d == leaving[g * half]:
            take(0, g)
        arrived(xin.at[source], rx_send.at[0], rx_recv.at[source])
        summed = (
            keep[0, slot]
            + pair_in[0, slot].astype(jnp.float32)
            + xin[source].astype(jnp.float32)
        ).astype(jnp.bfloat16)
        if d:
            outmail[source] = summed
            push(
                outmail.at[source], back.at[me], back_send.at[d], back_recv.at[me], source, tp
            )
        else:
            back[me] = summed
    for d in range(1, nsp):
        source = peer(d)
        arrived(back.at[source], back_send.at[0], back_recv.at[source])
    returned = back[...].reshape(nsp * cap, width)
    result = state[...]
    for j in range(picks.shape[0]):
        chosen = lax.dot_general(
            picks[j], returned, (((0,), (0,)), ((), ())), preferred_element_type=jnp.float32
        )
        result = result + wcol[j, :, 0:1] * chosen
    out_ref[...] = result.astype(out_ref.dtype)
    for copy in sent:
        copy.wait_send()


def pinned(array):
    return pltpu.with_memory_space_constraint(jnp.asarray(array), pltpu.MemorySpace.HBM)


def grid_tables(nsp, rows):
    count = HEAD_SIZE // 4
    inverse = theta_base ** (-np.arange(count, dtype=np.float64) * 2.0 / (HEAD_SIZE // 2))
    inverse = np.tile(inverse.astype(np.float32), 4)[None, :]

    def both(amount):
        angles = np.arange(amount, dtype=np.float32)[:, None] * inverse
        pair = [np.cos(angles), np.sin(angles)]
        return np.concatenate(pair, axis=1).astype(np.float32)

    lines = rows // GRID_W
    return both(nsp * lines).reshape(nsp, lines, 2 * HEAD_SIZE), both(GRID_W)


def on_device_fused(
    queries,
    keys,
    values,
    query_gain,
    key_norm_gain,
    out_weight,
    residual,
    norm_gain,
    expert_gate,
    expert_up,
    expert_down,
    routes,
    route_weight,
):
    nsp = lax.axis_size("sp")
    ntp = lax.axis_size("tp")
    rows = queries.shape[0]
    heads = queries.shape[1] // HEAD_SIZE
    own_rows, width = residual.shape
    top = routes.shape[1]
    cap = 2 * max(1, top * rows // (ntp * nsp))
    hidden_units = expert_gate.shape[2]
    by_row, by_column = grid_tables(nsp, rows)
    vmem = pl.BlockSpec(memory_space=pltpu.VMEM)
    hbm = pl.BlockSpec(memory_space=pltpu.MemorySpace.HBM)
    half, full = jnp.bfloat16, jnp.float32
    dma = pltpu.SemaphoreType.DMA
    return pl.pallas_call(
        functools.partial(layer_kernel, (nsp, ntp, heads, cap, rows, own_rows)),
        out_shape=jax.ShapeDtypeStruct((own_rows, width), half),
        in_specs=[hbm] * 15,
        out_specs=vmem,
        scratch_shapes=[
            pltpu.VMEM(by_row.shape[1:], full),
            pltpu.VMEM(by_column.shape, full),
            pltpu.VMEM(keys.shape, half),
            pltpu.VMEM((1, HEAD_SIZE), full),
            pltpu.VMEM(values.shape, half),
            pltpu.VMEM(queries.shape, half),
            pltpu.VMEM((1, HEAD_SIZE), full),
            pltpu.VMEM((top, own_rows), jnp.int32),
            pltpu.VMEM((top, own_rows), full),
            pltpu.VMEM((own_rows, width), half),
            pltpu.VMEM((1, width), full),
            pltpu.VMEM((top, nsp * cap, own_rows), half),
            pltpu.VMEM((nsp * cap, own_rows), half),
            pltpu.VMEM((top, own_rows, HEAD_SIZE), full),
            pltpu.VMEM(out_weight.shape, half),
            pltpu.VMEM(expert_gate.shape[1:], half),
            pltpu.VMEM(expert_up.shape[1:], half),
            pltpu.VMEM(expert_down.shape[1:], half),
            pltpu.VMEM((nsp, rows, 2 * HEAD_SIZE), half),
            pltpu.VMEM(queries.shape, half),
            pltpu.VMEM((ntp, own_rows, width), half),
            pltpu.VMEM((ntp, own_rows, width), half),
            pltpu.VMEM((own_rows, width), full),
            pltpu.VMEM((nsp, cap, width), half),
            pltpu.VMEM((ntp, nsp, cap, width), half),
            pltpu.VMEM((2 * nsp * cap, hidden_units), half),
            pltpu.VMEM((2, nsp, cap, width), full),
            pltpu.VMEM((2, nsp, cap, width), half),
            pltpu.VMEM((2, nsp, cap, width), half),
            pltpu.VMEM((nsp, cap, width), half),
            pltpu.VMEM((nsp, cap, width), half),
            pltpu.VMEM((nsp, cap, width), half),
            pltpu.VMEM((nsp, cap, width), half),
            dma((15,)),
            dma((nsp // 2,)),
            dma((nsp // 2,)),
            dma((nsp,)),
            dma((ntp,)),
            dma((ntp,)),
            dma((nsp,)),
            dma((nsp,)),
            dma((nsp,)),
            dma((nsp,)),
            dma((ntp, nsp)),
            dma((4,)),
            dma((4,)),
            dma((nsp,)),
            dma((nsp,)),
            dma((nsp,)),
            dma((nsp,)),
        ],
        compiler_params=pltpu.CompilerParams(
            collective_id=0, has_side_effects=True, vmem_limit_bytes=40_000_000
        ),
    )(
        *map(
            pinned,
            (
                by_row,
                by_column,
                keys,
                key_norm_gain[None, :],
                values,
                queries,
                query_gain[None, :],
                out_weight,
                routes.T,
                route_weight.T,
                residual,
                norm_gain[None, :],
                expert_gate,
                expert_up,
                expert_down,
            ),
        )
    )


def fits_fused(mesh):
    return mesh.shape["tp"] == 4 and mesh.shape["sp"] in (4, 8)


def solution(mesh):
    body = on_device_fused if fits_fused(mesh) else on_device
    placed = (
        P("sp", "tp"),
        P("sp", "tp"),
        P("sp", "tp"),
        P(),
        P(),
        P("tp", None),
        P(("sp", "tp"), None),
        P(),
        P("sp", None, "tp"),
        P("sp", None, "tp"),
        P("sp", "tp", None),
        P(("sp", "tp"), None),
        P(("sp", "tp"), None),
    )
    return jax.shard_map(
        body, mesh=mesh, in_specs=placed, out_specs=P(("sp", "tp"), None), check_vma=False
    )
```

```python
import functools
import math

import jax
import jax.numpy as jnp
import numpy as np
from jax import lax
from jax.experimental import pallas as pl
from jax.experimental.pallas import tpu as pltpu
from jax.sharding import PartitionSpec as P

HEAD_SIZE = 128
GRID_W = 64


norm_eps = 1e-06
theta_base = 10000.0


def head_normalize(packed, gain, heads):
    heads_float = packed.astype(jnp.float32).reshape(packed.shape[0], heads, HEAD_SIZE)
    scaled = heads_float * lax.rsqrt(
        jnp.mean(heads_float * heads_float, axis=-1, keepdims=True) + norm_eps
    )
    return scaled * gain


def rotary_tables(positions):
    freq_count = HEAD_SIZE // 4
    grid_row = (positions // GRID_W).astype(jnp.float32)
    grid_col = (positions % GRID_W).astype(jnp.float32)
    inverse = theta_base ** (-jnp.arange(freq_count, dtype=jnp.float32) * 2.0 / (HEAD_SIZE // 2))
    by_row = grid_row[:, None] * inverse
    by_col = grid_col[:, None] * inverse
    angles = jnp.concatenate([by_row, by_row, by_col, by_col], axis=-1)
    return (jnp.cos(angles), jnp.sin(angles))


def apply_rotation(heads_float, cosine_table, sine_values):
    freq_count = HEAD_SIZE // 4
    split_head = heads_float.reshape(heads_float.shape[:-1] + (2, 2, freq_count))
    turned = jnp.stack([-split_head[..., 1, :], split_head[..., 0, :]], axis=-2).reshape(
        heads_float.shape
    )
    return heads_float * cosine_table[:, None, :] + turned * sine_values[:, None, :]


def on_device(
    queries,
    keys,
    values,
    query_gain,
    key_norm_gain,
    out_weight,
    residual,
    norm_gain,
    expert_gate,
    expert_up,
    expert_down,
    routes,
    route_weight,
):
    local_rows = queries.shape[0]
    query_heads = queries.shape[1] // HEAD_SIZE
    key_heads = keys.shape[1] // HEAD_SIZE
    group_members = query_heads // key_heads
    score_scale = 1.0 / math.sqrt(HEAD_SIZE)
    positions = lax.axis_index("sp") * local_rows + jnp.arange(local_rows, dtype=jnp.int32)
    cosine_table, sine_values = rotary_tables(positions)
    rotated_queries = apply_rotation(
        head_normalize(queries, query_gain, query_heads), cosine_table, sine_values
    ).astype(jnp.bfloat16)
    query_block = rotated_queries.reshape(
        local_rows, key_heads, group_members, HEAD_SIZE
    ).transpose(1, 2, 0, 3)
    query_block = query_block.reshape(key_heads, group_members * local_rows, HEAD_SIZE)
    rotated_keys = apply_rotation(
        head_normalize(keys, key_norm_gain, key_heads), cosine_table, sine_values
    ).astype(jnp.bfloat16)
    rotated_keys = rotated_keys.reshape(local_rows, key_heads * HEAD_SIZE)
    start_state = (
        jnp.full((key_heads, group_members * local_rows), -1e30, jnp.float32),
        jnp.zeros((key_heads, group_members * local_rows), jnp.float32),
        jnp.zeros((key_heads, group_members * local_rows, HEAD_SIZE), jnp.float32),
    )
    folded = start_state
    key_piece = lax.all_gather(rotated_keys, "sp", axis=0, tiled=True)
    value_piece = lax.all_gather(values, "sp", axis=0, tiled=True)
    key_count = key_piece.shape[0]
    span_size = 512
    key_spans = key_piece.reshape(key_count // span_size, span_size, key_heads, HEAD_SIZE)
    value_spans = value_piece.reshape(key_count // span_size, span_size, key_heads, HEAD_SIZE)

    def one_span(state, span_pair):
        running, norm_sum, gathered_sum = state
        key_span, value_span = span_pair
        scores = (
            jnp.einsum("hqd,khd->hqk", query_block, key_span, preferred_element_type=jnp.float32)
            * score_scale
        )
        newest = jnp.maximum(running, jnp.max(scores, axis=-1))
        shrink = jnp.exp(running - newest)
        weights = jnp.exp(scores - newest[..., None])
        norm_sum = norm_sum * shrink + jnp.sum(weights, axis=-1)
        gathered_sum = gathered_sum * shrink[..., None] + jnp.einsum(
            "hqk,khd->hqd",
            weights.astype(jnp.bfloat16),
            value_span,
            preferred_element_type=jnp.float32,
        )
        return ((newest, norm_sum, gathered_sum), None)

    folded, _ = lax.scan(one_span, folded, (key_spans, value_spans))
    running, norm_sum, gathered_sum = folded
    attention = (gathered_sum / norm_sum[..., None]).reshape(
        key_heads, group_members, local_rows, HEAD_SIZE
    )
    attention = (
        attention.transpose(2, 0, 1, 3)
        .reshape(local_rows, query_heads * HEAD_SIZE)
        .astype(jnp.bfloat16)
    )
    out_rows = residual.shape[0]
    model_width = residual.shape[1]
    projected = lax.psum_scatter(
        jnp.dot(attention, out_weight, preferred_element_type=jnp.float32).astype(jnp.bfloat16),
        "tp",
        scatter_dimension=0,
        tiled=True,
    ).astype(jnp.float32)
    hidden_state = residual.astype(jnp.float32) + projected
    normed = (
        hidden_state
        * lax.rsqrt(jnp.mean(hidden_state * hidden_state, axis=-1, keepdims=True) + norm_eps)
        * norm_gain
    ).astype(jnp.bfloat16)
    route_top = routes.shape[1]
    group_width = lax.axis_size("tp")
    expert_count = lax.axis_size("sp") * expert_gate.shape[0]
    capacity = 2 * max(1, route_top * local_rows // (group_width * expert_count))
    flat_routes = routes.reshape(-1)
    onehot = (flat_routes[:, None] == jnp.arange(expert_count, dtype=jnp.int32)[None, :]).astype(
        jnp.int32
    )
    earlier = jnp.cumsum(onehot, axis=0) - onehot
    slot_rank = jnp.sum(earlier * onehot, axis=1)
    slot_index = flat_routes * capacity + slot_rank
    placer = (
        jnp.arange(expert_count * capacity, dtype=jnp.int32)[:, None] == slot_index[None, :]
    ).astype(jnp.bfloat16)
    route_rows = jnp.repeat(normed, route_top, axis=0)
    buffer = jnp.dot(placer, route_rows, preferred_element_type=jnp.float32).astype(jnp.bfloat16)
    buffer = buffer.reshape(expert_count, capacity, model_width)
    mail_rows = lax.all_to_all(buffer, "sp", split_axis=0, concat_axis=0, tiled=True)
    inbox_rows = lax.all_gather(mail_rows, "tp", axis=1, tiled=True)
    source_count = inbox_rows.shape[0]
    rows_in = inbox_rows.reshape(-1, model_width)
    gate_proj = jnp.dot(rows_in, expert_gate[0], preferred_element_type=jnp.float32)
    up_proj = jnp.dot(rows_in, expert_up[0], preferred_element_type=jnp.float32)
    hidden_act = (jax.nn.silu(gate_proj) * up_proj).astype(jnp.bfloat16)
    down_part = jnp.dot(hidden_act, expert_down[0], preferred_element_type=jnp.float32)
    down_part = down_part.reshape(source_count, group_width * capacity, model_width)
    summed = lax.psum_scatter(down_part.astype(jnp.bfloat16), "tp", scatter_dimension=1, tiled=True)
    returned = lax.all_to_all(summed, "sp", split_axis=0, concat_axis=0, tiled=True)
    per_route = jnp.dot(
        placer.T, returned.reshape(-1, model_width), preferred_element_type=jnp.float32
    )
    per_route = per_route.reshape(out_rows, route_top, model_width)
    moe_sum = jnp.sum(route_weight[:, :, None] * per_route, axis=1)
    return (hidden_state + moe_sum).astype(jnp.bfloat16)


MESH = pl.DeviceIdType.MESH
KV_ORDER = (1, 2, 4, 6)
ORDER = (0, 1, 2, 4, 3, 5, 6, 7)
O_GROUPS = ((0, 1, 2, 4), (3, 5, 6, 7))
A_GROUPS = ((0, 1, 2, 4), (3, 5, 6, 7))
LARGEST = 4
LEAVING = (4, 1, 2, 5, 3, 6, 7)
SCHEDULE = (
    ("spread", (0, 1, 2, 4), ()),
    ("weights", (), ()),
    ("settle_mate", (0,), ()),
    ("near", (0,), ((-1, "spread", (3, 5)),)),
    ("forward", (0, 1, 2, 4), ()),
    ("settle_diagonal", (0,), ()),
    ("far", (0,), ((-1, "spread", (6,)),)),
    ("spread", (7,), ()),
    ("cross", (4, 2, 1, 0), ()),
    ("settle_mate", (1,), ()),
    ("near", (1,), ((-1, "forward", (3, 5, 6)),)),
    ("forward", (7,), ()),
    ("settle_diagonal", (1,), ()),
    ("take", (0,), ()),
    ("far", (1,), ((-1, "finish", (4,)),)),
    ("cross", (7, 6, 5, 3), ()),
    ("finish", (2, 1, 0), ()),
    ("take", (1,), ()),
    ("finish", (7, 6, 5, 3), ()),
)
LOG2E = 1.4426950408889634


def layer_kernel(
    dims,
    row_hbm,
    column_hbm,
    k_hbm,
    kgain_hbm,
    v_hbm,
    q_hbm,
    qgain_hbm,
    wout_hbm,
    routes_hbm,
    weight_hbm,
    resid_hbm,
    ngain_hbm,
    gate_hbm,
    up_hbm,
    down_hbm,
    out_ref,
    row_ref,
    column_ref,
    k_ref,
    kgain_ref,
    q_ref,
    qgain_ref,
    routes_ref,
    weight_ref,
    resid_ref,
    ngain_ref,
    picks,
    placed_ref,
    wcol,
    wout,
    wgate,
    wup,
    wdown,
    k_all,
    v_all,
    probs,
    sums,
    att,
    part,
    rs_in,
    state,
    mail,
    inbox,
    hidden,
    keep,
    pair_out,
    pair_in,
    xsum,
    xin,
    outmail,
    back,
    wsem,
    gone,
    send_sem,
    k_recv,
    v_recv,
    rs_recv,
    mail_recv,
    mate_recv,
    x_recv,
    diagonal_recv,
    near_recv,
    far_recv,
    rx_recv,
    back_recv,
):
    nsp, ntp, heads, cap, rows, own_rows = dims
    width = out_ref.shape[1]
    me = lax.axis_index("sp")
    tp = lax.axis_index("tp")
    far = me // 2
    near = me % 2
    side = tp // 2
    core = tp % 2
    mate = side * 2 + (1 - core)
    across = (1 - side) * 2 + core
    diagonal = (1 - side) * 2 + (1 - core)
    twin = far * 2 + (1 - near)

    def flip(index, mask):
        value, bit = 0, 1
        while bit < nsp:
            digit = (index // bit) % 2
            value = value + bit * (1 - digit if mask & bit else digit)
            bit *= 2
        return value

    def peer(d):
        return flip(me, d)

    loads = []
    for i, (hbm, local) in enumerate(
        (
            (k_hbm, k_ref),
            (kgain_hbm, kgain_ref),
            (row_hbm.at[me], row_ref),
            (column_hbm, column_ref),
            (v_hbm, v_all.at[me]),
            (q_hbm, q_ref),
            (qgain_hbm, qgain_ref),
            (routes_hbm, routes_ref),
            (weight_hbm, weight_ref),
            (resid_hbm, resid_ref),
            (ngain_hbm, ngain_ref),
            (wout_hbm, wout),
            (gate_hbm.at[0], wgate),
            (up_hbm.at[0], wup),
            (down_hbm.at[0], wdown),
        )
    ):
        load = pltpu.make_async_copy(hbm, local, wsem.at[i])
        load.start()
        loads.append(load)

    barrier = pltpu.get_barrier_semaphore()
    for d in range(1, nsp):
        pl.semaphore_signal(barrier, inc=1, device_id=(peer(d), tp), device_id_type=MESH)
    for d in range(1, ntp):
        pl.semaphore_signal(
            barrier, inc=1, device_id=(me, lax.rem(tp + d, ntp)), device_id_type=MESH
        )

    sent = []

    def push(source, target, recv_sem, to_sp, to_tp):
        pltpu.make_async_remote_copy(
            src_ref=source,
            dst_ref=target,
            send_sem=send_sem.at[0],
            recv_sem=recv_sem,
            device_id=(to_sp, to_tp),
            device_id_type=MESH,
        ).start()
        sent.append(math.prod(source.shape))

    def arrived(target, recv_sem):
        pltpu.make_async_remote_copy(
            src_ref=target,
            dst_ref=target,
            send_sem=send_sem.at[0],
            recv_sem=recv_sem,
            device_id=(twin, tp),
            device_id_type=MESH,
        ).wait_recv()

    lane = lax.broadcasted_iota(jnp.int32, (1, HEAD_SIZE), 1)
    leading = lane % (HEAD_SIZE // 2) < HEAD_SIZE // 4

    def table(part):
        lanes = slice(part * HEAD_SIZE, (part + 1) * HEAD_SIZE)
        by_column = column_ref[:, lanes]
        return jnp.concatenate(
            [
                jnp.where(lane < HEAD_SIZE // 2, row_ref[k : k + 1, lanes], by_column)
                for k in range(row_ref.shape[0])
            ],
            axis=0,
        )

    def turned(head, gain_ref, tables):
        cosine, sine_a, sine_b = tables
        wide = head.astype(jnp.float32)
        scaled = wide * lax.rsqrt(jnp.mean(wide * wide, axis=-1, keepdims=True) + norm_eps)
        scaled = scaled * gain_ref[...]
        quarter = HEAD_SIZE // 4
        return (
            scaled * cosine
            + pltpu.roll(scaled, HEAD_SIZE - quarter, 1) * sine_a
            + pltpu.roll(scaled, quarter, 1) * sine_b
        ).astype(jnp.bfloat16)

    for i in (0, 1, 2, 3):
        loads[i].wait()
    sine = table(1)
    tables = (table(0), jnp.where(leading, -sine, 0.0), jnp.where(leading, 0.0, sine))
    k_all[me] = turned(k_ref[...], kgain_ref, tables)
    loads[4].wait()
    pl.semaphore_wait(barrier, nsp - 1 + ntp - 1)

    key_side = (k_all, k_recv)
    value_side = (v_all, v_recv)

    def offer(side):
        everyone, recv = side
        for d in KV_ORDER:
            arrival = recv.at[d // 2]
            push(everyone.at[me], everyone.at[me], arrival, peer(d), tp)

    def pass_on(side):
        everyone, recv = side
        for d in KV_ORDER:
            if d > 1:
                piece = everyone.at[peer(d)]
                arrived(piece, recv.at[d // 2])
                push(piece, piece, recv.at[0], twin, tp)

    def complete(side):
        everyone, recv = side
        arrived(everyone.at[pl.ds(0, nsp // 2)], recv.at[0])

    offer(key_side)
    offer(value_side)

    loads[5].wait()
    loads[6].wait()
    queries = [
        turned(q_ref[:, h * HEAD_SIZE : (h + 1) * HEAD_SIZE], qgain_ref, tables)
        for h in range(heads)
    ]
    for h in range(heads):
        att[:, h * HEAD_SIZE : (h + 1) * HEAD_SIZE] = queries[h]

    loads[7].wait()
    loads[8].wait()
    which = lax.broadcasted_iota(jnp.int32, (nsp, own_rows), 0)
    named = [which == routes_ref[j : j + 1, :] for j in range(routes_ref.shape[0])]
    named = [jnp.where(hit, 1.0, 0.0) for hit in named]
    hits = functools.reduce(jnp.add, named)
    square = (own_rows, own_rows)
    one, two = (lax.broadcasted_iota(jnp.int32, square, axis) for axis in (0, 1))
    rank = jnp.dot(
        hits.astype(jnp.bfloat16),
        jnp.where(one < two, 1.0, 0.0).astype(jnp.bfloat16),
        preferred_element_type=jnp.float32,
    )
    places = lax.broadcasted_iota(jnp.int32, (nsp, cap, own_rows), 1)
    ranked = jnp.where(places == rank.astype(jnp.int32)[:, None, :], 1.0, 0.0)
    placer = (ranked * hits[:, None, :]).reshape(nsp * cap, own_rows).astype(jnp.bfloat16)
    for j, hit in enumerate(named):
        picks[j] = (ranked * hit[:, None, :]).reshape(nsp * cap, own_rows).astype(jnp.bfloat16)
        column = jnp.sum(
            jnp.where(one == two, weight_ref[j : j + 1, :], 0.0), axis=1, keepdims=True
        )
        wcol[j] = jnp.broadcast_to(column, wcol.shape[1:])
    placed_ref[...] = placer

    pass_on(key_side)
    pass_on(value_side)
    complete(key_side)
    scale = LOG2E / math.sqrt(HEAD_SIZE)
    all_keys = k_all[...].reshape(nsp * rows, HEAD_SIZE)
    for h in range(heads):
        scores = lax.dot_general(
            att[:, h * HEAD_SIZE : (h + 1) * HEAD_SIZE],
            all_keys,
            (((1,), (1,)), ((), ())),
            preferred_element_type=jnp.float32,
        )
        top = jnp.max(scores, axis=-1, keepdims=True)
        weights = jnp.exp2((scores - top) * scale)
        sums[h] = jnp.broadcast_to(jnp.sum(weights, axis=-1, keepdims=True), sums.shape[1:])
        probs[h] = weights.astype(jnp.bfloat16)
    complete(value_side)
    all_values = v_all[...].reshape(nsp * rows, HEAD_SIZE)
    for h in range(heads):
        mixed = jnp.dot(probs[h], all_values, preferred_element_type=jnp.float32)
        att[:, h * HEAD_SIZE : (h + 1) * HEAD_SIZE] = (mixed / sums[h]).astype(jnp.bfloat16)

    loads[11].wait()
    tile = 512
    tiles = width // tile

    def tile_of(j):
        return pl.ds(j * tile, tile)

    strips = 2
    strip_width = width // strips

    def strip_of(j):
        return pl.ds(j * strip_width, strip_width)

    for j in range(tiles):
        columns = slice(j * tile, (j + 1) * tile)
        product = jnp.dot(att[...], wout[:, columns], preferred_element_type=jnp.float32)
        part[:, :, columns] = product.astype(jnp.bfloat16).reshape(ntp, own_rows, tile)
        if (j + 1) % (tiles // strips) == 0:
            i = j // (tiles // strips)
            push(
                part.at[diagonal, :, strip_of(i)],
                rs_in.at[1, :, strip_of(i)],
                rs_recv.at[1 + i],
                me,
                mate,
            )
    push(part.at[mate], rs_in.at[2], rs_recv.at[0], me, mate)
    for j in range(strips):
        columns = slice(j * strip_width, (j + 1) * strip_width)
        arrived(rs_in.at[1, :, strip_of(j)], rs_recv.at[1 + j])
        part[across, :, columns] = (
            part[across, :, columns].astype(jnp.float32)
            + rs_in[1, :, columns].astype(jnp.float32)
        ).astype(jnp.bfloat16)
        push(
            part.at[across, :, strip_of(j)],
            rs_in.at[3, :, strip_of(j)],
            rs_recv.at[1 + strips + j],
            me,
            across,
        )
    loads[9].wait()
    loads[10].wait()
    arrived(rs_in.at[2], rs_recv.at[0])
    squares = jnp.zeros((own_rows, 1), jnp.float32)
    for j in range(strips):
        columns = slice(j * strip_width, (j + 1) * strip_width)
        early = (
            resid_ref[:, columns].astype(jnp.float32)
            + part[tp, :, columns].astype(jnp.float32)
            + rs_in[2, :, columns].astype(jnp.float32)
        )
        arrived(rs_in.at[3, :, strip_of(j)], rs_recv.at[1 + strips + j])
        total = early + rs_in[3, :, columns].astype(jnp.float32)
        squares = squares + jnp.sum(total * total, axis=-1, keepdims=True)
        state[:, columns] = total
    normed = (state[...] * lax.rsqrt(squares / width + norm_eps) * ngain_ref[...]).astype(
        jnp.bfloat16
    )
    mail[...] = (
        jnp.dot(placed_ref[...], normed, preferred_element_type=jnp.float32)
        .astype(jnp.bfloat16)
        .reshape(nsp, cap, width)
    )
    for d in LEAVING:
        to = peer(d)
        push(mail.at[to], inbox.at[tp, me], mail_recv.at[d], to, tp)
    inbox[tp, me] = mail[me]

    def group_of(groups, d):
        return next(g for g, group in enumerate(groups) if d in group)

    def spread(*pieces):
        for d in pieces:
            piece = inbox.at[tp, peer(d)]
            if d:
                arrived(piece, mail_recv.at[d])
            push(piece, piece, x_recv.at[d], me, across)
            push(piece, piece, mate_recv.at[group_of(O_GROUPS, d)], me, mate)

    def forward(*pieces):
        for d in pieces:
            piece = inbox.at[across, peer(d)]
            arrived(piece, x_recv.at[d])
            push(piece, piece, diagonal_recv.at[group_of(A_GROUPS, d)], me, mate)

    def settle_mate(g):
        arrived(inbox.at[mate, pl.ds(0, len(O_GROUPS[g]))], mate_recv.at[g])

    def settle_diagonal(g):
        arrived(inbox.at[diagonal, pl.ds(0, len(A_GROUPS[g]))], diagonal_recv.at[g])

    def runs_of(pieces):
        slots = sorted(ORDER.index(d) for d in pieces)
        starts = [slot for slot in slots if slot - 1 not in slots]
        ends = [slot + 1 for slot in slots if slot + 1 not in slots]
        return list(zip(starts, ends))

    def in_order(pieces):
        return sorted(pieces, key=ORDER.index)

    fine = 256

    def experts(parts, pieces, hooks):
        pieces = in_order(pieces)
        blocks = [(owner, peer(d)) for owner, _ in parts for d in pieces]
        live = len(blocks) * cap

        @pl.loop(0, wgate.shape[1] // fine)
        def _(j):
            columns = pl.ds(pl.multiple_of(j * fine, fine), fine)
            block = jnp.concatenate([inbox[owner, source] for owner, source in blocks], axis=0)
            gate = jnp.dot(block, wgate[:, columns], preferred_element_type=jnp.float32)
            up = jnp.dot(block, wup[:, columns], preferred_element_type=jnp.float32)
            hidden[:live, columns] = (gate / (1.0 + jnp.exp(-gate)) * up).astype(jnp.bfloat16)

        hooks(-1)
        for j in range(tiles):
            columns = slice(j * tile, (j + 1) * tile)
            product = jnp.dot(hidden[:live], wdown[:, columns], preferred_element_type=jnp.float32)
            product = product.reshape(len(parts), len(pieces), cap, tile)
            for i, (_, target) in enumerate(parts):
                done = 0
                for start, end in runs_of(pieces):
                    count = end - start
                    target[start:end, :, columns] = product[i, done : done + count].astype(
                        target.dtype
                    )
                    done += count
            hooks(j)

    def strip(ref, start, end, j):
        return ref.at[pl.ds(start, end - start), :, tile_of(j)]

    def hand(i, pieces, arrival, j):
        for start, end in runs_of(pieces):
            push(
                strip(pair_out.at[i], start, end, j),
                strip(pair_in.at[i], start, end, j),
                arrival,
                me,
                mate,
            )

    def take(i, pieces, arrival):
        arrived(pair_in.at[i, pl.ds(0, len(pieces))], arrival)

    def near_side(g, hooks):
        pieces = O_GROUPS[g]

        def each(j):
            if j >= 0:
                hand(0, pieces, near_recv.at[g], j)
            hooks(j)

        experts([(tp, keep.at[0]), (mate, pair_out.at[0])], pieces, each)

    def far_side(g, hooks):
        pieces = A_GROUPS[g]

        def each(j):
            if j >= 0:
                hand(1, pieces, far_recv.at[g], j)
            hooks(j)

        experts([(diagonal, pair_out.at[1]), (across, keep.at[1])], pieces, each)

    def cross(*order):
        g = group_of(A_GROUPS, order[0])
        take(1, A_GROUPS[g], far_recv.at[g])
        for d in order:
            slot = ORDER.index(d)
            xsum[slot] = (keep[1, slot] + pair_in[1, slot].astype(jnp.float32)).astype(
                jnp.bfloat16
            )
            push(xsum.at[slot], xin.at[slot], rx_recv.at[slot], me, across)

    def finish(*pieces):
        for d in pieces:
            slot = ORDER.index(d)
            source = peer(d)
            arrived(xin.at[slot], rx_recv.at[slot])
            summed = (
                keep[0, slot]
                + pair_in[0, slot].astype(jnp.float32)
                + xin[slot].astype(jnp.float32)
            ).astype(jnp.bfloat16)
            if d:
                outmail[slot] = summed
                push(outmail.at[slot], back.at[me], back_recv.at[0], source, tp)
            else:
                back[me] = summed

    def plan(steps):
        table = {}
        for at, action in steps:
            table.setdefault(at, []).append(action)

        def run(j):
            for action in table.get(j, ()):
                action()

        return run

    def later(function, *given):
        return lambda: function(*given)

    def weights_here():
        for i in (12, 13, 14):
            loads[i].wait()

    simple = {
        "spread": spread,
        "forward": forward,
        "finish": finish,
        "settle_mate": settle_mate,
        "settle_diagonal": settle_diagonal,
        "weights": weights_here,
        "cross": cross,
        "take": lambda g: take(0, O_GROUPS[g], near_recv.at[g]),
    }
    for kind, given, hooks in SCHEDULE:
        if kind in simple:
            simple[kind](*given)
            continue
        run = plan([(at, later(simple[what], *pieces)) for at, what, pieces in hooks])
        (near_side if kind == "near" else far_side)(*given, run)
    arrived(back.at[pl.ds(0, nsp - 1)], back_recv.at[0])
    for j in range(tiles):
        columns = slice(j * tile, (j + 1) * tile)
        returned = back[:, :, columns].reshape(nsp * cap, tile)
        result = state[:, columns]
        for i in range(picks.shape[0]):
            chosen = lax.dot_general(
                picks[i], returned, (((0,), (0,)), ((), ())), preferred_element_type=jnp.float32
            )
            result = result + wcol[i, :, 0:1] * chosen
        out_ref[:, columns] = result.astype(out_ref.dtype)
    assert sum(sent) == math.prod(gone.shape)
    pltpu.make_async_remote_copy(
        src_ref=gone,
        dst_ref=gone,
        send_sem=send_sem.at[0],
        recv_sem=back_recv.at[0],
        device_id=(twin, tp),
        device_id_type=MESH,
    ).wait_send()


def pinned(array):
    return pltpu.with_memory_space_constraint(jnp.asarray(array), pltpu.MemorySpace.HBM)


def grid_tables(nsp, rows):
    count = HEAD_SIZE // 4
    inverse = theta_base ** (-np.arange(count, dtype=np.float64) * 2.0 / (HEAD_SIZE // 2))
    inverse = np.tile(inverse.astype(np.float32), 4)[None, :]

    def both(amount):
        angles = np.arange(amount, dtype=np.float32)[:, None] * inverse
        pair = [np.cos(angles), np.sin(angles)]
        return np.concatenate(pair, axis=1).astype(np.float32)

    lines = rows // GRID_W
    return both(nsp * lines).reshape(nsp, lines, 2 * HEAD_SIZE), both(GRID_W)


def sent_rows(nsp, ntp, rows, own_rows, cap, width):
    attention = 2 * (nsp - 1) * rows * HEAD_SIZE // width
    return attention + (ntp - 1) * own_rows + (2 * (nsp - 1) + 6 * nsp) * cap


def on_device_fused(
    queries,
    keys,
    values,
    query_gain,
    key_norm_gain,
    out_weight,
    residual,
    norm_gain,
    expert_gate,
    expert_up,
    expert_down,
    routes,
    route_weight,
):
    nsp = lax.axis_size("sp")
    ntp = lax.axis_size("tp")
    rows = queries.shape[0]
    heads = queries.shape[1] // HEAD_SIZE
    own_rows, width = residual.shape
    top = routes.shape[1]
    cap = 2 * max(1, top * rows // (ntp * nsp))
    hidden_units = expert_gate.shape[2]
    by_row, by_column = grid_tables(nsp, rows)
    vmem = pl.BlockSpec(memory_space=pltpu.VMEM)
    hbm = pl.BlockSpec(memory_space=pltpu.MemorySpace.HBM)
    half, full = jnp.bfloat16, jnp.float32
    dma = pltpu.SemaphoreType.DMA
    return pl.pallas_call(
        functools.partial(layer_kernel, (nsp, ntp, heads, cap, rows, own_rows)),
        out_shape=jax.ShapeDtypeStruct((own_rows, width), half),
        in_specs=[hbm] * 15,
        out_specs=vmem,
        scratch_shapes=[
            pltpu.VMEM(by_row.shape[1:], full),
            pltpu.VMEM(by_column.shape, full),
            pltpu.VMEM(keys.shape, half),
            pltpu.VMEM((1, HEAD_SIZE), full),
            pltpu.VMEM(queries.shape, half),
            pltpu.VMEM((1, HEAD_SIZE), full),
            pltpu.VMEM((top, own_rows), jnp.int32),
            pltpu.VMEM((top, own_rows), full),
            pltpu.VMEM((own_rows, width), half),
            pltpu.VMEM((1, width), full),
            pltpu.VMEM((top, nsp * cap, own_rows), half),
            pltpu.VMEM((nsp * cap, own_rows), half),
            pltpu.VMEM((top, own_rows, HEAD_SIZE), full),
            pltpu.VMEM(out_weight.shape, half),
            pltpu.VMEM(expert_gate.shape[1:], half),
            pltpu.VMEM(expert_up.shape[1:], half),
            pltpu.VMEM(expert_down.shape[1:], half),
            pltpu.VMEM((nsp, rows, HEAD_SIZE), half),
            pltpu.VMEM((nsp, rows, HEAD_SIZE), half),
            pltpu.VMEM((heads, rows, nsp * rows), half),
            pltpu.VMEM((heads, rows, HEAD_SIZE), full),
            pltpu.VMEM(queries.shape, half),
            pltpu.VMEM((ntp, own_rows, width), half),
            pltpu.VMEM((ntp, own_rows, width), half),
            pltpu.VMEM((own_rows, width), full),
            pltpu.VMEM((nsp, cap, width), half),
            pltpu.VMEM((ntp, nsp, cap, width), half),
            pltpu.VMEM((2 * LARGEST * cap, hidden_units), half),
            pltpu.VMEM((2, nsp, cap, width), full),
            pltpu.VMEM((2, nsp, cap, width), half),
            pltpu.VMEM((2, nsp, cap, width), half),
            pltpu.VMEM((nsp, cap, width), half),
            pltpu.VMEM((nsp, cap, width), half),
            pltpu.VMEM((nsp, cap, width), half),
            pltpu.VMEM((nsp, cap, width), half),
            dma((15,)),
            pltpu.VMEM((sent_rows(nsp, ntp, rows, own_rows, cap, width), width), half),
            dma((1,)),
            dma((nsp // 2,)),
            dma((nsp // 2,)),
            dma((5,)),
            dma((nsp,)),
            dma((len(O_GROUPS),)),
            dma((nsp,)),
            dma((len(A_GROUPS),)),
            dma((len(O_GROUPS),)),
            dma((len(A_GROUPS),)),
            dma((nsp,)),
            dma((1,)),
        ],
        compiler_params=pltpu.CompilerParams(
            collective_id=0, has_side_effects=True, vmem_limit_bytes=40_000_000
        ),
    )(
        *map(
            pinned,
            (
                by_row,
                by_column,
                keys,
                key_norm_gain[None, :],
                values,
                queries,
                query_gain[None, :],
                out_weight,
                routes.T,
                route_weight.T,
                residual,
                norm_gain[None, :],
                expert_gate,
                expert_up,
                expert_down,
            ),
        )
    )


def fits_fused(mesh):
    return mesh.shape["tp"] == 4 and mesh.shape["sp"] == 8


def solution(mesh):
    body = on_device_fused if fits_fused(mesh) else on_device
    placed = (
        P("sp", "tp"),
        P("sp", "tp"),
        P("sp", "tp"),
        P(),
        P(),
        P("tp", None),
        P(("sp", "tp"), None),
        P(),
        P("sp", None, "tp"),
        P("sp", None, "tp"),
        P("sp", "tp", None),
        P(("sp", "tp"), None),
        P(("sp", "tp"), None),
    )
    return jax.shard_map(
        body, mesh=mesh, in_specs=placed, out_specs=P(("sp", "tp"), None), check_vma=False
    )
```

```python
import functools
import math

import jax
import jax.numpy as jnp
import numpy as np
from jax import lax
from jax.experimental import pallas as pl
from jax.experimental.pallas import tpu as pltpu
from jax.sharding import PartitionSpec as P

HEAD_SIZE = 128
GRID_W = 64


norm_eps = 1e-06
theta_base = 10000.0


def head_normalize(packed, gain, heads):
    heads_float = packed.astype(jnp.float32).reshape(packed.shape[0], heads, HEAD_SIZE)
    scaled = heads_float * lax.rsqrt(
        jnp.mean(heads_float * heads_float, axis=-1, keepdims=True) + norm_eps
    )
    return scaled * gain


def rotary_tables(positions):
    freq_count = HEAD_SIZE // 4
    grid_row = (positions // GRID_W).astype(jnp.float32)
    grid_col = (positions % GRID_W).astype(jnp.float32)
    inverse = theta_base ** (-jnp.arange(freq_count, dtype=jnp.float32) * 2.0 / (HEAD_SIZE // 2))
    by_row = grid_row[:, None] * inverse
    by_col = grid_col[:, None] * inverse
    angles = jnp.concatenate([by_row, by_row, by_col, by_col], axis=-1)
    return (jnp.cos(angles), jnp.sin(angles))


def apply_rotation(heads_float, cosine_table, sine_values):
    freq_count = HEAD_SIZE // 4
    split_head = heads_float.reshape(heads_float.shape[:-1] + (2, 2, freq_count))
    turned = jnp.stack([-split_head[..., 1, :], split_head[..., 0, :]], axis=-2).reshape(
        heads_float.shape
    )
    return heads_float * cosine_table[:, None, :] + turned * sine_values[:, None, :]


def on_device(
    queries,
    keys,
    values,
    query_gain,
    key_norm_gain,
    out_weight,
    residual,
    norm_gain,
    expert_gate,
    expert_up,
    expert_down,
    routes,
    route_weight,
):
    local_rows = queries.shape[0]
    query_heads = queries.shape[1] // HEAD_SIZE
    key_heads = keys.shape[1] // HEAD_SIZE
    group_members = query_heads // key_heads
    score_scale = 1.0 / math.sqrt(HEAD_SIZE)
    positions = lax.axis_index("sp") * local_rows + jnp.arange(local_rows, dtype=jnp.int32)
    cosine_table, sine_values = rotary_tables(positions)
    rotated_queries = apply_rotation(
        head_normalize(queries, query_gain, query_heads), cosine_table, sine_values
    ).astype(jnp.bfloat16)
    query_block = rotated_queries.reshape(
        local_rows, key_heads, group_members, HEAD_SIZE
    ).transpose(1, 2, 0, 3)
    query_block = query_block.reshape(key_heads, group_members * local_rows, HEAD_SIZE)
    rotated_keys = apply_rotation(
        head_normalize(keys, key_norm_gain, key_heads), cosine_table, sine_values
    ).astype(jnp.bfloat16)
    rotated_keys = rotated_keys.reshape(local_rows, key_heads * HEAD_SIZE)
    start_state = (
        jnp.full((key_heads, group_members * local_rows), -1e30, jnp.float32),
        jnp.zeros((key_heads, group_members * local_rows), jnp.float32),
        jnp.zeros((key_heads, group_members * local_rows, HEAD_SIZE), jnp.float32),
    )
    folded = start_state
    key_piece = lax.all_gather(rotated_keys, "sp", axis=0, tiled=True)
    value_piece = lax.all_gather(values, "sp", axis=0, tiled=True)
    key_count = key_piece.shape[0]
    span_size = 512
    key_spans = key_piece.reshape(key_count // span_size, span_size, key_heads, HEAD_SIZE)
    value_spans = value_piece.reshape(key_count // span_size, span_size, key_heads, HEAD_SIZE)

    def one_span(state, span_pair):
        running, norm_sum, gathered_sum = state
        key_span, value_span = span_pair
        scores = (
            jnp.einsum("hqd,khd->hqk", query_block, key_span, preferred_element_type=jnp.float32)
            * score_scale
        )
        newest = jnp.maximum(running, jnp.max(scores, axis=-1))
        shrink = jnp.exp(running - newest)
        weights = jnp.exp(scores - newest[..., None])
        norm_sum = norm_sum * shrink + jnp.sum(weights, axis=-1)
        gathered_sum = gathered_sum * shrink[..., None] + jnp.einsum(
            "hqk,khd->hqd",
            weights.astype(jnp.bfloat16),
            value_span,
            preferred_element_type=jnp.float32,
        )
        return ((newest, norm_sum, gathered_sum), None)

    folded, _ = lax.scan(one_span, folded, (key_spans, value_spans))
    running, norm_sum, gathered_sum = folded
    attention = (gathered_sum / norm_sum[..., None]).reshape(
        key_heads, group_members, local_rows, HEAD_SIZE
    )
    attention = (
        attention.transpose(2, 0, 1, 3)
        .reshape(local_rows, query_heads * HEAD_SIZE)
        .astype(jnp.bfloat16)
    )
    out_rows = residual.shape[0]
    model_width = residual.shape[1]
    projected = lax.psum_scatter(
        jnp.dot(attention, out_weight, preferred_element_type=jnp.float32).astype(jnp.bfloat16),
        "tp",
        scatter_dimension=0,
        tiled=True,
    ).astype(jnp.float32)
    hidden_state = residual.astype(jnp.float32) + projected
    normed = (
        hidden_state
        * lax.rsqrt(jnp.mean(hidden_state * hidden_state, axis=-1, keepdims=True) + norm_eps)
        * norm_gain
    ).astype(jnp.bfloat16)
    route_top = routes.shape[1]
    group_width = lax.axis_size("tp")
    expert_count = lax.axis_size("sp") * expert_gate.shape[0]
    capacity = 2 * max(1, route_top * local_rows // (group_width * expert_count))
    flat_routes = routes.reshape(-1)
    onehot = (flat_routes[:, None] == jnp.arange(expert_count, dtype=jnp.int32)[None, :]).astype(
        jnp.int32
    )
    earlier = jnp.cumsum(onehot, axis=0) - onehot
    slot_rank = jnp.sum(earlier * onehot, axis=1)
    slot_index = flat_routes * capacity + slot_rank
    placer = (
        jnp.arange(expert_count * capacity, dtype=jnp.int32)[:, None] == slot_index[None, :]
    ).astype(jnp.bfloat16)
    route_rows = jnp.repeat(normed, route_top, axis=0)
    buffer = jnp.dot(placer, route_rows, preferred_element_type=jnp.float32).astype(jnp.bfloat16)
    buffer = buffer.reshape(expert_count, capacity, model_width)
    mail_rows = lax.all_to_all(buffer, "sp", split_axis=0, concat_axis=0, tiled=True)
    inbox_rows = lax.all_gather(mail_rows, "tp", axis=1, tiled=True)
    source_count = inbox_rows.shape[0]
    rows_in = inbox_rows.reshape(-1, model_width)
    gate_proj = jnp.dot(rows_in, expert_gate[0], preferred_element_type=jnp.float32)
    up_proj = jnp.dot(rows_in, expert_up[0], preferred_element_type=jnp.float32)
    hidden_act = (jax.nn.silu(gate_proj) * up_proj).astype(jnp.bfloat16)
    down_part = jnp.dot(hidden_act, expert_down[0], preferred_element_type=jnp.float32)
    down_part = down_part.reshape(source_count, group_width * capacity, model_width)
    summed = lax.psum_scatter(down_part.astype(jnp.bfloat16), "tp", scatter_dimension=1, tiled=True)
    returned = lax.all_to_all(summed, "sp", split_axis=0, concat_axis=0, tiled=True)
    per_route = jnp.dot(
        placer.T, returned.reshape(-1, model_width), preferred_element_type=jnp.float32
    )
    per_route = per_route.reshape(out_rows, route_top, model_width)
    moe_sum = jnp.sum(route_weight[:, :, None] * per_route, axis=1)
    return (hidden_state + moe_sum).astype(jnp.bfloat16)


MESH = pl.DeviceIdType.MESH
KV_ORDER = (4, 1, 2)
KV_SLOT = {1: 0, 2: 1, 4: 2}
KV_RELAY = ((4, (3, 2, 1)), (2, (1,)))
ORDER = (0, 1, 2, 4, 3, 5, 6, 7)
O_GROUPS = ((0, 1, 2, 4), (3, 5, 6, 7))
A_GROUPS = ((0, 1, 2, 4), (3, 5), (6, 7))
LARGEST = 4
LEAVING = (4, 1, 2, 5, 3, 6, 7)
SCHEDULE = (
    ("spread", (0, 1, 2, 4), ()),
    ("weights", (), ()),
    ("settle_mate", (0,), ()),
    ("near", (0,), ((-3, "forward", (0,)), (-2, "spread", (3,)), (-1, "forward", (1, 2)), (1, "spread", (5,)))),
    ("forward", (4,), ()),
    ("settle_diagonal", (0,), ()),
    ("far", (0,), ((-2, "spread", (6,)), (-1, "forward", (3, 5)))),
    ("spread", (7,), ()),
    ("settle_diagonal", (1,), ()),
    ("far", (1,), ((-2, "take_far", (0,)), (-2, "cross", (4, 2)), (2, "forward", (6,)))),
    ("settle_mate", (1,), ()),
    ("near", (1,), ((-2, "take_far", (1,)), (-2, "cross", (5, 3)), (-1, "forward", (7,)))),
    ("take_near", (0,), ()),
    ("finish", (4,), ()),
    ("settle_diagonal", (2,), ()),
    ("far", (2,), ((-1, "finish", (2,)),)),
    ("take_near", (1,), ()),
    ("finish", (5,), ()),
    ("take_far", (2,), ()),
    ("cross", (7, 6, 1, 0), ()),
    ("finish", (3, 7, 6, 1, 0), ()),
)
LOG2E = 1.4426950408889634


def layer_kernel(
    dims,
    row_hbm,
    column_hbm,
    k_hbm,
    kgain_hbm,
    v_hbm,
    q_hbm,
    qgain_hbm,
    wout_hbm,
    routes_hbm,
    weight_hbm,
    resid_hbm,
    ngain_hbm,
    gate_hbm,
    up_hbm,
    down_hbm,
    out_ref,
    row_ref,
    column_ref,
    k_ref,
    kgain_ref,
    q_ref,
    qgain_ref,
    routes_ref,
    weight_ref,
    resid_ref,
    ngain_ref,
    picks,
    placed_ref,
    wcol,
    wout,
    wgate,
    wup,
    wdown,
    k_all,
    v_all,
    probs,
    sums,
    att,
    part,
    rs_in,
    state,
    mail,
    inbox,
    hidden,
    keep,
    pair_out,
    pair_in,
    xsum,
    xin,
    outmail,
    back,
    wsem,
    gone,
    send_sem,
    k_recv,
    v_recv,
    rs_recv,
    mail_recv,
    mate_recv,
    x_recv,
    diagonal_recv,
    near_recv,
    far_recv,
    rx_recv,
    back_recv,
):
    nsp, ntp, heads, cap, rows, own_rows = dims
    width = out_ref.shape[1]
    me = lax.axis_index("sp")
    tp = lax.axis_index("tp")
    far = me // 2
    near = me % 2
    side = tp // 2
    core = tp % 2
    mate = side * 2 + (1 - core)
    across = (1 - side) * 2 + core
    diagonal = (1 - side) * 2 + (1 - core)
    twin = far * 2 + (1 - near)

    def flip(index, mask):
        value, bit = 0, 1
        while bit < nsp:
            digit = (index // bit) % 2
            value = value + bit * (1 - digit if mask & bit else digit)
            bit *= 2
        return value

    def peer(d):
        return flip(me, d)

    loads = []
    for i, (hbm, local) in enumerate(
        (
            (k_hbm, k_ref),
            (kgain_hbm, kgain_ref),
            (row_hbm.at[me], row_ref),
            (column_hbm, column_ref),
            (v_hbm, v_all.at[me]),
            (q_hbm, q_ref),
            (qgain_hbm, qgain_ref),
            (routes_hbm, routes_ref),
            (weight_hbm, weight_ref),
            (resid_hbm, resid_ref),
            (ngain_hbm, ngain_ref),
            (wout_hbm, wout),
            (gate_hbm.at[0], wgate),
            (up_hbm.at[0], wup),
            (down_hbm.at[0], wdown),
        )
    ):
        load = pltpu.make_async_copy(hbm, local, wsem.at[i])
        load.start()
        loads.append(load)

    barrier = pltpu.get_barrier_semaphore()
    for d in range(1, nsp):
        pl.semaphore_signal(barrier, inc=1, device_id=(peer(d), tp), device_id_type=MESH)
    for d in range(1, ntp):
        pl.semaphore_signal(
            barrier, inc=1, device_id=(me, lax.rem(tp + d, ntp)), device_id_type=MESH
        )

    sent = []

    def push(source, target, recv_sem, to_sp, to_tp):
        pltpu.make_async_remote_copy(
            src_ref=source,
            dst_ref=target,
            send_sem=send_sem.at[0],
            recv_sem=recv_sem,
            device_id=(to_sp, to_tp),
            device_id_type=MESH,
        ).start()
        sent.append(math.prod(source.shape))

    def arrived(target, recv_sem):
        pltpu.make_async_remote_copy(
            src_ref=target,
            dst_ref=target,
            send_sem=send_sem.at[0],
            recv_sem=recv_sem,
            device_id=(twin, tp),
            device_id_type=MESH,
        ).wait_recv()

    lane = lax.broadcasted_iota(jnp.int32, (1, HEAD_SIZE), 1)
    leading = lane % (HEAD_SIZE // 2) < HEAD_SIZE // 4

    def table(part):
        lanes = slice(part * HEAD_SIZE, (part + 1) * HEAD_SIZE)
        by_column = column_ref[:, lanes]
        return jnp.concatenate(
            [
                jnp.where(lane < HEAD_SIZE // 2, row_ref[k : k + 1, lanes], by_column)
                for k in range(row_ref.shape[0])
            ],
            axis=0,
        )

    def turned(head, gain_ref, tables):
        cosine, sine_a, sine_b = tables
        wide = head.astype(jnp.float32)
        scaled = wide * lax.rsqrt(jnp.mean(wide * wide, axis=-1, keepdims=True) + norm_eps)
        scaled = scaled * gain_ref[...]
        quarter = HEAD_SIZE // 4
        return (
            scaled * cosine
            + pltpu.roll(scaled, HEAD_SIZE - quarter, 1) * sine_a
            + pltpu.roll(scaled, quarter, 1) * sine_b
        ).astype(jnp.bfloat16)

    for i in (0, 1, 2, 3):
        loads[i].wait()
    sine = table(1)
    tables = (table(0), jnp.where(leading, -sine, 0.0), jnp.where(leading, 0.0, sine))
    k_all[me] = turned(k_ref[...], kgain_ref, tables)
    loads[4].wait()
    pl.semaphore_wait(barrier, nsp - 1 + ntp - 1)

    key_side = (k_all, k_recv)
    value_side = (v_all, v_recv)

    half = nsp // 2

    def offer(side):
        everyone, recv = side
        for d in KV_ORDER:
            push(everyone.at[me], everyone.at[me], recv.at[KV_SLOT[d]], peer(d), tp)

    def pass_on(side):
        everyone, recv = side
        for d, onward in KV_RELAY:
            piece = everyone.at[peer(d)]
            arrived(piece, recv.at[KV_SLOT[d]])
            for to in onward:
                push(piece, piece, recv.at[0], peer(to), tp)

    def complete(side):
        everyone, recv = side
        arrived(everyone.at[pl.ds(0, nsp - 1 - len(KV_RELAY))], recv.at[0])

    offer(key_side)
    offer(value_side)

    loads[5].wait()
    loads[6].wait()
    queries = [
        turned(q_ref[:, h * HEAD_SIZE : (h + 1) * HEAD_SIZE], qgain_ref, tables)
        for h in range(heads)
    ]
    for h in range(heads):
        att[:, h * HEAD_SIZE : (h + 1) * HEAD_SIZE] = queries[h]

    loads[7].wait()
    loads[8].wait()
    which = lax.broadcasted_iota(jnp.int32, (nsp, own_rows), 0)
    named = [which == routes_ref[j : j + 1, :] for j in range(routes_ref.shape[0])]
    named = [jnp.where(hit, 1.0, 0.0) for hit in named]
    hits = functools.reduce(jnp.add, named)
    square = (own_rows, own_rows)
    one, two = (lax.broadcasted_iota(jnp.int32, square, axis) for axis in (0, 1))
    rank = jnp.dot(
        hits.astype(jnp.bfloat16),
        jnp.where(one < two, 1.0, 0.0).astype(jnp.bfloat16),
        preferred_element_type=jnp.float32,
    )
    places = lax.broadcasted_iota(jnp.int32, (nsp, cap, own_rows), 1)
    ranked = jnp.where(places == rank.astype(jnp.int32)[:, None, :], 1.0, 0.0)
    placer = (ranked * hits[:, None, :]).reshape(nsp * cap, own_rows).astype(jnp.bfloat16)
    for j, hit in enumerate(named):
        picks[j] = (ranked * hit[:, None, :]).reshape(nsp * cap, own_rows).astype(jnp.bfloat16)
        column = jnp.sum(
            jnp.where(one == two, weight_ref[j : j + 1, :], 0.0), axis=1, keepdims=True
        )
        wcol[j] = jnp.broadcast_to(column, wcol.shape[1:])
    placed_ref[...] = placer

    pass_on(key_side)
    pass_on(value_side)
    complete(key_side)
    scale = LOG2E / math.sqrt(HEAD_SIZE)
    all_keys = k_all[...].reshape(nsp * rows, HEAD_SIZE)
    for h in range(heads):
        scores = lax.dot_general(
            att[:, h * HEAD_SIZE : (h + 1) * HEAD_SIZE],
            all_keys,
            (((1,), (1,)), ((), ())),
            preferred_element_type=jnp.float32,
        )
        top = jnp.max(scores, axis=-1, keepdims=True)
        weights = jnp.exp2((scores - top) * scale)
        sums[h] = jnp.broadcast_to(jnp.sum(weights, axis=-1, keepdims=True), sums.shape[1:])
        probs[h] = weights.astype(jnp.bfloat16)
    complete(value_side)
    all_values = v_all[...].reshape(nsp * rows, HEAD_SIZE)
    for h in range(heads):
        mixed = jnp.dot(probs[h], all_values, preferred_element_type=jnp.float32)
        att[:, h * HEAD_SIZE : (h + 1) * HEAD_SIZE] = (mixed / sums[h]).astype(jnp.bfloat16)

    loads[11].wait()
    tile = 512
    tiles = width // tile

    def tile_of(j):
        return pl.ds(j * tile, tile)

    strips = 2
    strip_width = width // strips

    def strip_of(j):
        return pl.ds(j * strip_width, strip_width)

    for j in range(tiles):
        columns = slice(j * tile, (j + 1) * tile)
        product = jnp.dot(att[...], wout[:, columns], preferred_element_type=jnp.float32)
        part[:, :, columns] = product.astype(jnp.bfloat16).reshape(ntp, own_rows, tile)
        if (j + 1) % (tiles // strips) == 0:
            i = j // (tiles // strips)
            push(
                part.at[diagonal, :, strip_of(i)],
                rs_in.at[1, :, strip_of(i)],
                rs_recv.at[1 + i],
                me,
                mate,
            )
    push(part.at[mate], rs_in.at[2], rs_recv.at[0], me, mate)
    for j in range(strips):
        columns = slice(j * strip_width, (j + 1) * strip_width)
        arrived(rs_in.at[1, :, strip_of(j)], rs_recv.at[1 + j])
        part[across, :, columns] = (
            part[across, :, columns].astype(jnp.float32)
            + rs_in[1, :, columns].astype(jnp.float32)
        ).astype(jnp.bfloat16)
        push(
            part.at[across, :, strip_of(j)],
            rs_in.at[3, :, strip_of(j)],
            rs_recv.at[1 + strips + j],
            me,
            across,
        )
    loads[9].wait()
    loads[10].wait()
    arrived(rs_in.at[2], rs_recv.at[0])
    squares = jnp.zeros((own_rows, 1), jnp.float32)
    for j in range(strips):
        columns = slice(j * strip_width, (j + 1) * strip_width)
        early = (
            resid_ref[:, columns].astype(jnp.float32)
            + part[tp, :, columns].astype(jnp.float32)
            + rs_in[2, :, columns].astype(jnp.float32)
        )
        arrived(rs_in.at[3, :, strip_of(j)], rs_recv.at[1 + strips + j])
        total = early + rs_in[3, :, columns].astype(jnp.float32)
        squares = squares + jnp.sum(total * total, axis=-1, keepdims=True)
        state[:, columns] = total
    normed = (state[...] * lax.rsqrt(squares / width + norm_eps) * ngain_ref[...]).astype(
        jnp.bfloat16
    )
    mail[...] = (
        jnp.dot(placed_ref[...], normed, preferred_element_type=jnp.float32)
        .astype(jnp.bfloat16)
        .reshape(nsp, cap, width)
    )
    for d in LEAVING:
        to = peer(d)
        push(mail.at[to], inbox.at[tp, me], mail_recv.at[d], to, tp)
    inbox[tp, me] = mail[me]

    def group_of(groups, d):
        return next(g for g, group in enumerate(groups) if d in group)

    def spread(*pieces):
        for d in pieces:
            piece = inbox.at[tp, peer(d)]
            if d:
                arrived(piece, mail_recv.at[d])
            push(piece, piece, x_recv.at[d], me, across)
            push(piece, piece, mate_recv.at[group_of(O_GROUPS, d)], me, mate)

    def forward(*pieces):
        for d in pieces:
            piece = inbox.at[across, peer(d)]
            arrived(piece, x_recv.at[d])
            push(piece, piece, diagonal_recv.at[group_of(A_GROUPS, d)], me, mate)

    def settle_mate(g):
        arrived(inbox.at[mate, pl.ds(0, len(O_GROUPS[g]))], mate_recv.at[g])

    def settle_diagonal(g):
        arrived(inbox.at[diagonal, pl.ds(0, len(A_GROUPS[g]))], diagonal_recv.at[g])

    def runs_of(pieces):
        slots = sorted(ORDER.index(d) for d in pieces)
        starts = [slot for slot in slots if slot - 1 not in slots]
        ends = [slot + 1 for slot in slots if slot + 1 not in slots]
        return list(zip(starts, ends))

    def in_order(pieces):
        return sorted(pieces, key=ORDER.index)

    fine = 256

    def experts(parts, pieces, hooks):
        pieces = in_order(pieces)
        blocks = [(owner, peer(d)) for owner, _ in parts for d in pieces]
        live = len(blocks) * cap

        steps = wgate.shape[1] // fine
        for j in range(steps):
            columns = slice(j * fine, (j + 1) * fine)
            block = jnp.concatenate([inbox[owner, source] for owner, source in blocks], axis=0)
            gate = jnp.dot(block, wgate[:, columns], preferred_element_type=jnp.float32)
            up = jnp.dot(block, wup[:, columns], preferred_element_type=jnp.float32)
            hidden[:live, columns] = (gate / (1.0 + jnp.exp(-gate)) * up).astype(jnp.bfloat16)
            hooks(j - steps)

        for j in range(tiles):
            columns = slice(j * tile, (j + 1) * tile)
            product = jnp.dot(hidden[:live], wdown[:, columns], preferred_element_type=jnp.float32)
            product = product.reshape(len(parts), len(pieces), cap, tile)
            for i, (_, target) in enumerate(parts):
                done = 0
                for start, end in runs_of(pieces):
                    count = end - start
                    target[start:end, :, columns] = product[i, done : done + count].astype(
                        target.dtype
                    )
                    done += count
            hooks(j)

    def strip(ref, start, end, j):
        return ref.at[pl.ds(start, end - start), :, tile_of(j)]

    def hand(i, pieces, arrival, j):
        for start, end in runs_of(pieces):
            push(
                strip(pair_out.at[i], start, end, j),
                strip(pair_in.at[i], start, end, j),
                arrival,
                me,
                mate,
            )

    def take(i, pieces, arrival):
        arrived(pair_in.at[i, pl.ds(0, len(pieces))], arrival)

    def near_side(g, hooks):
        pieces = O_GROUPS[g]

        def each(j):
            if j >= 0:
                hand(0, pieces, near_recv.at[g], j)
            hooks(j)

        experts([(tp, keep.at[0]), (mate, pair_out.at[0])], pieces, each)

    def far_side(g, hooks):
        pieces = A_GROUPS[g]

        def each(j):
            if j >= 0:
                hand(1, pieces, far_recv.at[g], j)
            hooks(j)

        experts([(diagonal, pair_out.at[1]), (across, keep.at[1])], pieces, each)

    def cross(*order):
        for d in order:
            slot = ORDER.index(d)
            xsum[slot] = (keep[1, slot] + pair_in[1, slot].astype(jnp.float32)).astype(
                jnp.bfloat16
            )
            push(xsum.at[slot], xin.at[slot], rx_recv.at[slot], me, across)

    def finish(*pieces):
        for d in pieces:
            slot = ORDER.index(d)
            source = peer(d)
            arrived(xin.at[slot], rx_recv.at[slot])
            summed = (
                keep[0, slot]
                + pair_in[0, slot].astype(jnp.float32)
                + xin[slot].astype(jnp.float32)
            ).astype(jnp.bfloat16)
            if d:
                outmail[slot] = summed
                push(outmail.at[slot], back.at[me], back_recv.at[0], source, tp)
            else:
                back[me] = summed

    def plan(steps):
        table = {}
        for at, action in steps:
            table.setdefault(at, []).append(action)

        def run(j):
            for action in table.get(j, ()):
                action()

        return run

    def later(function, *given):
        return lambda: function(*given)

    def weights_here():
        for i in (12, 13, 14):
            loads[i].wait()

    simple = {
        "spread": spread,
        "forward": forward,
        "finish": finish,
        "settle_mate": settle_mate,
        "settle_diagonal": settle_diagonal,
        "weights": weights_here,
        "cross": cross,
        "take_near": lambda g: take(0, O_GROUPS[g], near_recv.at[g]),
        "take_far": lambda g: take(1, A_GROUPS[g], far_recv.at[g]),
    }
    for kind, given, hooks in SCHEDULE:
        if kind in simple:
            simple[kind](*given)
            continue
        run = plan([(at, later(simple[what], *pieces)) for at, what, pieces in hooks])
        (near_side if kind == "near" else far_side)(*given, run)
    arrived(back.at[pl.ds(0, nsp - 1)], back_recv.at[0])
    for j in range(tiles):
        columns = slice(j * tile, (j + 1) * tile)
        returned = back[:, :, columns].reshape(nsp * cap, tile)
        result = state[:, columns]
        for i in range(picks.shape[0]):
            chosen = lax.dot_general(
                picks[i], returned, (((0,), (0,)), ((), ())), preferred_element_type=jnp.float32
            )
            result = result + wcol[i, :, 0:1] * chosen
        out_ref[:, columns] = result.astype(out_ref.dtype)
    assert sum(sent) == math.prod(gone.shape)
    pltpu.make_async_remote_copy(
        src_ref=gone,
        dst_ref=gone,
        send_sem=send_sem.at[0],
        recv_sem=back_recv.at[0],
        device_id=(twin, tp),
        device_id_type=MESH,
    ).wait_send()


def pinned(array):
    return pltpu.with_memory_space_constraint(jnp.asarray(array), pltpu.MemorySpace.HBM)


def grid_tables(nsp, rows):
    count = HEAD_SIZE // 4
    inverse = theta_base ** (-np.arange(count, dtype=np.float64) * 2.0 / (HEAD_SIZE // 2))
    inverse = np.tile(inverse.astype(np.float32), 4)[None, :]

    def both(amount):
        angles = np.arange(amount, dtype=np.float32)[:, None] * inverse
        pair = [np.cos(angles), np.sin(angles)]
        return np.concatenate(pair, axis=1).astype(np.float32)

    lines = rows // GRID_W
    return both(nsp * lines).reshape(nsp, lines, 2 * HEAD_SIZE), both(GRID_W)


def sent_rows(nsp, ntp, rows, own_rows, cap, width):
    attention = 2 * (nsp - 1) * rows * HEAD_SIZE // width
    return attention + (ntp - 1) * own_rows + (2 * (nsp - 1) + 6 * nsp) * cap


def on_device_fused(
    queries,
    keys,
    values,
    query_gain,
    key_norm_gain,
    out_weight,
    residual,
    norm_gain,
    expert_gate,
    expert_up,
    expert_down,
    routes,
    route_weight,
):
    nsp = lax.axis_size("sp")
    ntp = lax.axis_size("tp")
    rows = queries.shape[0]
    heads = queries.shape[1] // HEAD_SIZE
    own_rows, width = residual.shape
    top = routes.shape[1]
    cap = 2 * max(1, top * rows // (ntp * nsp))
    hidden_units = expert_gate.shape[2]
    by_row, by_column = grid_tables(nsp, rows)
    vmem = pl.BlockSpec(memory_space=pltpu.VMEM)
    hbm = pl.BlockSpec(memory_space=pltpu.MemorySpace.HBM)
    half, full = jnp.bfloat16, jnp.float32
    dma = pltpu.SemaphoreType.DMA
    return pl.pallas_call(
        functools.partial(layer_kernel, (nsp, ntp, heads, cap, rows, own_rows)),
        out_shape=jax.ShapeDtypeStruct((own_rows, width), half),
        in_specs=[hbm] * 15,
        out_specs=vmem,
        scratch_shapes=[
            pltpu.VMEM(by_row.shape[1:], full),
            pltpu.VMEM(by_column.shape, full),
            pltpu.VMEM(keys.shape, half),
            pltpu.VMEM((1, HEAD_SIZE), full),
            pltpu.VMEM(queries.shape, half),
            pltpu.VMEM((1, HEAD_SIZE), full),
            pltpu.VMEM((top, own_rows), jnp.int32),
            pltpu.VMEM((top, own_rows), full),
            pltpu.VMEM((own_rows, width), half),
            pltpu.VMEM((1, width), full),
            pltpu.VMEM((top, nsp * cap, own_rows), half),
            pltpu.VMEM((nsp * cap, own_rows), half),
            pltpu.VMEM((top, own_rows, HEAD_SIZE), full),
            pltpu.VMEM(out_weight.shape, half),
            pltpu.VMEM(expert_gate.shape[1:], half),
            pltpu.VMEM(expert_up.shape[1:], half),
            pltpu.VMEM(expert_down.shape[1:], half),
            pltpu.VMEM((nsp, rows, HEAD_SIZE), half),
            pltpu.VMEM((nsp, rows, HEAD_SIZE), half),
            pltpu.VMEM((heads, rows, nsp * rows), half),
            pltpu.VMEM((heads, rows, HEAD_SIZE), full),
            pltpu.VMEM(queries.shape, half),
            pltpu.VMEM((ntp, own_rows, width), half),
            pltpu.VMEM((ntp, own_rows, width), half),
            pltpu.VMEM((own_rows, width), full),
            pltpu.VMEM((nsp, cap, width), half),
            pltpu.VMEM((ntp, nsp, cap, width), half),
            pltpu.VMEM((2 * LARGEST * cap, hidden_units), half),
            pltpu.VMEM((2, nsp, cap, width), full),
            pltpu.VMEM((2, nsp, cap, width), half),
            pltpu.VMEM((2, nsp, cap, width), half),
            pltpu.VMEM((nsp, cap, width), half),
            pltpu.VMEM((nsp, cap, width), half),
            pltpu.VMEM((nsp, cap, width), half),
            pltpu.VMEM((nsp, cap, width), half),
            dma((15,)),
            pltpu.VMEM((sent_rows(nsp, ntp, rows, own_rows, cap, width), width), half),
            dma((1,)),
            dma((3,)),
            dma((3,)),
            dma((5,)),
            dma((nsp,)),
            dma((len(O_GROUPS),)),
            dma((nsp,)),
            dma((len(A_GROUPS),)),
            dma((len(O_GROUPS),)),
            dma((len(A_GROUPS),)),
            dma((nsp,)),
            dma((1,)),
        ],
        compiler_params=pltpu.CompilerParams(
            collective_id=0, has_side_effects=True, vmem_limit_bytes=40_000_000
        ),
    )(
        *map(
            pinned,
            (
                by_row,
                by_column,
                keys,
                key_norm_gain[None, :],
                values,
                queries,
                query_gain[None, :],
                out_weight,
                routes.T,
                route_weight.T,
                residual,
                norm_gain[None, :],
                expert_gate,
                expert_up,
                expert_down,
            ),
        )
    )


def fits_fused(mesh):
    return mesh.shape["tp"] == 4 and mesh.shape["sp"] == 8


def solution(mesh):
    body = on_device_fused if fits_fused(mesh) else on_device
    placed = (
        P("sp", "tp"),
        P("sp", "tp"),
        P("sp", "tp"),
        P(),
        P(),
        P("tp", None),
        P(("sp", "tp"), None),
        P(),
        P("sp", None, "tp"),
        P("sp", None, "tp"),
        P("sp", "tp", None),
        P(("sp", "tp"), None),
        P(("sp", "tp"), None),
    )
    return jax.shard_map(
        body, mesh=mesh, in_specs=placed, out_specs=P(("sp", "tp"), None), check_vma=False
    )
```

```python
import functools
import math

import jax
import jax.numpy as jnp
import numpy as np
from jax import lax
from jax.experimental import pallas as pl
from jax.experimental.pallas import tpu as pltpu
from jax.sharding import PartitionSpec as P

HEAD_SIZE = 128
GRID_W = 64


norm_eps = 1e-06
theta_base = 10000.0


def head_normalize(packed, gain, heads):
    heads_float = packed.astype(jnp.float32).reshape(packed.shape[0], heads, HEAD_SIZE)
    scaled = heads_float * lax.rsqrt(
        jnp.mean(heads_float * heads_float, axis=-1, keepdims=True) + norm_eps
    )
    return scaled * gain


def rotary_tables(positions):
    freq_count = HEAD_SIZE // 4
    grid_row = (positions // GRID_W).astype(jnp.float32)
    grid_col = (positions % GRID_W).astype(jnp.float32)
    inverse = theta_base ** (-jnp.arange(freq_count, dtype=jnp.float32) * 2.0 / (HEAD_SIZE // 2))
    by_row = grid_row[:, None] * inverse
    by_col = grid_col[:, None] * inverse
    angles = jnp.concatenate([by_row, by_row, by_col, by_col], axis=-1)
    return (jnp.cos(angles), jnp.sin(angles))


def apply_rotation(heads_float, cosine_table, sine_values):
    freq_count = HEAD_SIZE // 4
    split_head = heads_float.reshape(heads_float.shape[:-1] + (2, 2, freq_count))
    turned = jnp.stack([-split_head[..., 1, :], split_head[..., 0, :]], axis=-2).reshape(
        heads_float.shape
    )
    return heads_float * cosine_table[:, None, :] + turned * sine_values[:, None, :]


def on_device(
    queries,
    keys,
    values,
    query_gain,
    key_norm_gain,
    out_weight,
    residual,
    norm_gain,
    expert_gate,
    expert_up,
    expert_down,
    routes,
    route_weight,
):
    local_rows = queries.shape[0]
    query_heads = queries.shape[1] // HEAD_SIZE
    key_heads = keys.shape[1] // HEAD_SIZE
    group_members = query_heads // key_heads
    score_scale = 1.0 / math.sqrt(HEAD_SIZE)
    positions = lax.axis_index("sp") * local_rows + jnp.arange(local_rows, dtype=jnp.int32)
    cosine_table, sine_values = rotary_tables(positions)
    rotated_queries = apply_rotation(
        head_normalize(queries, query_gain, query_heads), cosine_table, sine_values
    ).astype(jnp.bfloat16)
    query_block = rotated_queries.reshape(
        local_rows, key_heads, group_members, HEAD_SIZE
    ).transpose(1, 2, 0, 3)
    query_block = query_block.reshape(key_heads, group_members * local_rows, HEAD_SIZE)
    rotated_keys = apply_rotation(
        head_normalize(keys, key_norm_gain, key_heads), cosine_table, sine_values
    ).astype(jnp.bfloat16)
    rotated_keys = rotated_keys.reshape(local_rows, key_heads * HEAD_SIZE)
    start_state = (
        jnp.full((key_heads, group_members * local_rows), -1e30, jnp.float32),
        jnp.zeros((key_heads, group_members * local_rows), jnp.float32),
        jnp.zeros((key_heads, group_members * local_rows, HEAD_SIZE), jnp.float32),
    )
    folded = start_state
    key_piece = lax.all_gather(rotated_keys, "sp", axis=0, tiled=True)
    value_piece = lax.all_gather(values, "sp", axis=0, tiled=True)
    key_count = key_piece.shape[0]
    span_size = 512
    key_spans = key_piece.reshape(key_count // span_size, span_size, key_heads, HEAD_SIZE)
    value_spans = value_piece.reshape(key_count // span_size, span_size, key_heads, HEAD_SIZE)

    def one_span(state, span_pair):
        running, norm_sum, gathered_sum = state
        key_span, value_span = span_pair
        scores = (
            jnp.einsum("hqd,khd->hqk", query_block, key_span, preferred_element_type=jnp.float32)
            * score_scale
        )
        newest = jnp.maximum(running, jnp.max(scores, axis=-1))
        shrink = jnp.exp(running - newest)
        weights = jnp.exp(scores - newest[..., None])
        norm_sum = norm_sum * shrink + jnp.sum(weights, axis=-1)
        gathered_sum = gathered_sum * shrink[..., None] + jnp.einsum(
            "hqk,khd->hqd",
            weights.astype(jnp.bfloat16),
            value_span,
            preferred_element_type=jnp.float32,
        )
        return ((newest, norm_sum, gathered_sum), None)

    folded, _ = lax.scan(one_span, folded, (key_spans, value_spans))
    running, norm_sum, gathered_sum = folded
    attention = (gathered_sum / norm_sum[..., None]).reshape(
        key_heads, group_members, local_rows, HEAD_SIZE
    )
    attention = (
        attention.transpose(2, 0, 1, 3)
        .reshape(local_rows, query_heads * HEAD_SIZE)
        .astype(jnp.bfloat16)
    )
    out_rows = residual.shape[0]
    model_width = residual.shape[1]
    projected = lax.psum_scatter(
        jnp.dot(attention, out_weight, preferred_element_type=jnp.float32).astype(jnp.bfloat16),
        "tp",
        scatter_dimension=0,
        tiled=True,
    ).astype(jnp.float32)
    hidden_state = residual.astype(jnp.float32) + projected
    normed = (
        hidden_state
        * lax.rsqrt(jnp.mean(hidden_state * hidden_state, axis=-1, keepdims=True) + norm_eps)
        * norm_gain
    ).astype(jnp.bfloat16)
    route_top = routes.shape[1]
    group_width = lax.axis_size("tp")
    expert_count = lax.axis_size("sp") * expert_gate.shape[0]
    capacity = 2 * max(1, route_top * local_rows // (group_width * expert_count))
    flat_routes = routes.reshape(-1)
    onehot = (flat_routes[:, None] == jnp.arange(expert_count, dtype=jnp.int32)[None, :]).astype(
        jnp.int32
    )
    earlier = jnp.cumsum(onehot, axis=0) - onehot
    slot_rank = jnp.sum(earlier * onehot, axis=1)
    slot_index = flat_routes * capacity + slot_rank
    placer = (
        jnp.arange(expert_count * capacity, dtype=jnp.int32)[:, None] == slot_index[None, :]
    ).astype(jnp.bfloat16)
    route_rows = jnp.repeat(normed, route_top, axis=0)
    buffer = jnp.dot(placer, route_rows, preferred_element_type=jnp.float32).astype(jnp.bfloat16)
    buffer = buffer.reshape(expert_count, capacity, model_width)
    mail_rows = lax.all_to_all(buffer, "sp", split_axis=0, concat_axis=0, tiled=True)
    inbox_rows = lax.all_gather(mail_rows, "tp", axis=1, tiled=True)
    source_count = inbox_rows.shape[0]
    rows_in = inbox_rows.reshape(-1, model_width)
    gate_proj = jnp.dot(rows_in, expert_gate[0], preferred_element_type=jnp.float32)
    up_proj = jnp.dot(rows_in, expert_up[0], preferred_element_type=jnp.float32)
    hidden_act = (jax.nn.silu(gate_proj) * up_proj).astype(jnp.bfloat16)
    down_part = jnp.dot(hidden_act, expert_down[0], preferred_element_type=jnp.float32)
    down_part = down_part.reshape(source_count, group_width * capacity, model_width)
    summed = lax.psum_scatter(down_part.astype(jnp.bfloat16), "tp", scatter_dimension=1, tiled=True)
    returned = lax.all_to_all(summed, "sp", split_axis=0, concat_axis=0, tiled=True)
    per_route = jnp.dot(
        placer.T, returned.reshape(-1, model_width), preferred_element_type=jnp.float32
    )
    per_route = per_route.reshape(out_rows, route_top, model_width)
    moe_sum = jnp.sum(route_weight[:, :, None] * per_route, axis=1)
    return (hidden_state + moe_sum).astype(jnp.bfloat16)


MESH = pl.DeviceIdType.MESH
KV_ORDER = (4, 1, 2)
KV_SLOT = {1: 0, 2: 1, 4: 2}
KV_RELAY = ((4, (3, 2, 1)), (2, (1,)))
ORDER = (0, 1, 2, 4, 3, 5, 6, 7)
O_GROUPS = ((0, 1, 2, 4), (3, 5, 6, 7))
A_GROUPS = ((0, 1, 2, 4), (3, 5), (6, 7))
LARGEST = 4
LEAVING = (4, 1, 2, 5, 3, 6, 7)
SCHEDULE = (
    ("spread", (0, 1, 2, 4), ()),
    ("weights", (), ()),
    ("settle_mate", (0,), ()),
    ("near", (0,), ((-3, "forward", (0,)), (-2, "spread", (3,)), (-1, "forward", (1, 2)), (1, "spread", (5,)))),
    ("forward", (4,), ()),
    ("settle_diagonal", (0,), ()),
    ("far", (0,), ((-2, "spread", (6,)), (-1, "forward", (3, 5)))),
    ("spread", (7,), ()),
    ("settle_diagonal", (1,), ()),
    ("far", (1,), ((-2, "take_far", (0,)), (-2, "cross", (4, 2)), (2, "forward", (6,)))),
    ("settle_mate", (1,), ()),
    ("near", (1,), ((-2, "take_far", (1,)), (-2, "cross", (5, 3)), (-1, "forward", (7,)))),
    ("take_near", (0,), ()),
    ("finish", (4,), ()),
    ("settle_diagonal", (2,), ()),
    ("far", (2,), ((-1, "finish", (2,)),)),
    ("take_near", (1,), ()),
    ("finish", (5,), ()),
    ("take_half", (0,), ()),
    ("cross_half", (0, 7, 6), ()),
    ("take_half", (1,), ()),
    ("cross_half", (1, 7, 6), ()),
    ("cross", (1, 0), ()),
    ("finish", (3,), ()),
    ("finish_half", (0, 7, 6), ()),
    ("finish_half", (1, 7, 6), ()),
    ("finish", (1, 0), ()),
)
LOG2E = 1.4426950408889634


def layer_kernel(
    dims,
    row_hbm,
    column_hbm,
    k_hbm,
    kgain_hbm,
    v_hbm,
    q_hbm,
    qgain_hbm,
    wout_hbm,
    routes_hbm,
    weight_hbm,
    resid_hbm,
    ngain_hbm,
    gate_hbm,
    up_hbm,
    down_hbm,
    out_ref,
    row_ref,
    column_ref,
    k_ref,
    kgain_ref,
    q_ref,
    qgain_ref,
    routes_ref,
    weight_ref,
    resid_ref,
    ngain_ref,
    picks,
    placed_ref,
    wcol,
    wout,
    wgate,
    wup,
    wdown,
    k_all,
    v_all,
    probs,
    sums,
    att,
    part,
    rs_in,
    state,
    mail,
    inbox,
    hidden,
    keep,
    pair_out,
    pair_in,
    xsum,
    xin,
    outmail,
    back,
    wsem,
    gone,
    send_sem,
    k_recv,
    v_recv,
    rs_recv,
    mail_recv,
    mate_recv,
    x_recv,
    diagonal_recv,
    near_recv,
    far_recv,
    rx_recv,
    back_recv,
):
    nsp, ntp, heads, cap, rows, own_rows = dims
    width = out_ref.shape[1]
    me = lax.axis_index("sp")
    tp = lax.axis_index("tp")
    far = me // 2
    near = me % 2
    side = tp // 2
    core = tp % 2
    mate = side * 2 + (1 - core)
    across = (1 - side) * 2 + core
    diagonal = (1 - side) * 2 + (1 - core)
    twin = far * 2 + (1 - near)

    def flip(index, mask):
        value, bit = 0, 1
        while bit < nsp:
            digit = (index // bit) % 2
            value = value + bit * (1 - digit if mask & bit else digit)
            bit *= 2
        return value

    def peer(d):
        return flip(me, d)

    loads = []
    for i, (hbm, local) in enumerate(
        (
            (k_hbm, k_ref),
            (kgain_hbm, kgain_ref),
            (row_hbm.at[me], row_ref),
            (column_hbm, column_ref),
            (v_hbm, v_all.at[me]),
            (q_hbm, q_ref),
            (qgain_hbm, qgain_ref),
            (routes_hbm, routes_ref),
            (weight_hbm, weight_ref),
            (resid_hbm, resid_ref),
            (ngain_hbm, ngain_ref),
            (wout_hbm, wout),
            (gate_hbm.at[0], wgate),
            (up_hbm.at[0], wup),
            (down_hbm.at[0], wdown),
        )
    ):
        load = pltpu.make_async_copy(hbm, local, wsem.at[i])
        load.start()
        loads.append(load)

    barrier = pltpu.get_barrier_semaphore()
    for d in range(1, nsp):
        pl.semaphore_signal(barrier, inc=1, device_id=(peer(d), tp), device_id_type=MESH)
    for d in range(1, ntp):
        pl.semaphore_signal(
            barrier, inc=1, device_id=(me, lax.rem(tp + d, ntp)), device_id_type=MESH
        )

    sent = []

    def push(source, target, recv_sem, to_sp, to_tp):
        pltpu.make_async_remote_copy(
            src_ref=source,
            dst_ref=target,
            send_sem=send_sem.at[0],
            recv_sem=recv_sem,
            device_id=(to_sp, to_tp),
            device_id_type=MESH,
        ).start()
        sent.append(math.prod(source.shape))

    def arrived(target, recv_sem):
        pltpu.make_async_remote_copy(
            src_ref=target,
            dst_ref=target,
            send_sem=send_sem.at[0],
            recv_sem=recv_sem,
            device_id=(twin, tp),
            device_id_type=MESH,
        ).wait_recv()

    lane = lax.broadcasted_iota(jnp.int32, (1, HEAD_SIZE), 1)
    leading = lane % (HEAD_SIZE // 2) < HEAD_SIZE // 4

    def table(part):
        lanes = slice(part * HEAD_SIZE, (part + 1) * HEAD_SIZE)
        by_column = column_ref[:, lanes]
        return jnp.concatenate(
            [
                jnp.where(lane < HEAD_SIZE // 2, row_ref[k : k + 1, lanes], by_column)
                for k in range(row_ref.shape[0])
            ],
            axis=0,
        )

    def turned(head, gain_ref, tables):
        cosine, sine_a, sine_b = tables
        wide = head.astype(jnp.float32)
        scaled = wide * lax.rsqrt(jnp.mean(wide * wide, axis=-1, keepdims=True) + norm_eps)
        scaled = scaled * gain_ref[...]
        quarter = HEAD_SIZE // 4
        return (
            scaled * cosine
            + pltpu.roll(scaled, HEAD_SIZE - quarter, 1) * sine_a
            + pltpu.roll(scaled, quarter, 1) * sine_b
        ).astype(jnp.bfloat16)

    for i in (0, 1, 2, 3):
        loads[i].wait()
    sine = table(1)
    tables = (table(0), jnp.where(leading, -sine, 0.0), jnp.where(leading, 0.0, sine))
    k_all[me] = turned(k_ref[...], kgain_ref, tables)
    loads[4].wait()
    pl.semaphore_wait(barrier, nsp - 1 + ntp - 1)

    key_side = (k_all, k_recv)
    value_side = (v_all, v_recv)

    half = nsp // 2

    def offer(side):
        everyone, recv = side
        for d in KV_ORDER:
            push(everyone.at[me], everyone.at[me], recv.at[KV_SLOT[d]], peer(d), tp)

    def pass_on(side):
        everyone, recv = side
        for d, onward in KV_RELAY:
            piece = everyone.at[peer(d)]
            arrived(piece, recv.at[KV_SLOT[d]])
            for to in onward:
                push(piece, piece, recv.at[0], peer(to), tp)

    def complete(side):
        everyone, recv = side
        arrived(everyone.at[pl.ds(0, nsp - 1 - len(KV_RELAY))], recv.at[0])

    offer(key_side)
    offer(value_side)

    loads[5].wait()
    loads[6].wait()
    queries = [
        turned(q_ref[:, h * HEAD_SIZE : (h + 1) * HEAD_SIZE], qgain_ref, tables)
        for h in range(heads)
    ]
    for h in range(heads):
        att[:, h * HEAD_SIZE : (h + 1) * HEAD_SIZE] = queries[h]

    loads[7].wait()
    loads[8].wait()
    which = lax.broadcasted_iota(jnp.int32, (nsp, own_rows), 0)
    named = [which == routes_ref[j : j + 1, :] for j in range(routes_ref.shape[0])]
    named = [jnp.where(hit, 1.0, 0.0) for hit in named]
    hits = functools.reduce(jnp.add, named)
    square = (own_rows, own_rows)
    one, two = (lax.broadcasted_iota(jnp.int32, square, axis) for axis in (0, 1))
    rank = jnp.dot(
        hits.astype(jnp.bfloat16),
        jnp.where(one < two, 1.0, 0.0).astype(jnp.bfloat16),
        preferred_element_type=jnp.float32,
    )
    places = lax.broadcasted_iota(jnp.int32, (nsp, cap, own_rows), 1)
    ranked = jnp.where(places == rank.astype(jnp.int32)[:, None, :], 1.0, 0.0)
    placer = (ranked * hits[:, None, :]).reshape(nsp * cap, own_rows).astype(jnp.bfloat16)
    for j, hit in enumerate(named):
        picks[j] = (ranked * hit[:, None, :]).reshape(nsp * cap, own_rows).astype(jnp.bfloat16)
        column = jnp.sum(
            jnp.where(one == two, weight_ref[j : j + 1, :], 0.0), axis=1, keepdims=True
        )
        wcol[j] = jnp.broadcast_to(column, wcol.shape[1:])
    placed_ref[...] = placer

    pass_on(key_side)
    pass_on(value_side)
    complete(key_side)
    scale = LOG2E / math.sqrt(HEAD_SIZE)
    all_keys = k_all[...].reshape(nsp * rows, HEAD_SIZE)
    for h in range(heads):
        scores = lax.dot_general(
            att[:, h * HEAD_SIZE : (h + 1) * HEAD_SIZE],
            all_keys,
            (((1,), (1,)), ((), ())),
            preferred_element_type=jnp.float32,
        )
        top = jnp.max(scores, axis=-1, keepdims=True)
        weights = jnp.exp2((scores - top) * scale)
        sums[h] = jnp.broadcast_to(jnp.sum(weights, axis=-1, keepdims=True), sums.shape[1:])
        probs[h] = weights.astype(jnp.bfloat16)
    complete(value_side)
    all_values = v_all[...].reshape(nsp * rows, HEAD_SIZE)
    for h in range(heads):
        mixed = jnp.dot(probs[h], all_values, preferred_element_type=jnp.float32)
        att[:, h * HEAD_SIZE : (h + 1) * HEAD_SIZE] = (mixed / sums[h]).astype(jnp.bfloat16)

    loads[11].wait()
    tile = 512
    tiles = width // tile

    def tile_of(j):
        return pl.ds(j * tile, tile)

    strips = 2
    strip_width = width // strips

    def strip_of(j):
        return pl.ds(j * strip_width, strip_width)

    for j in range(tiles):
        columns = slice(j * tile, (j + 1) * tile)
        product = jnp.dot(att[...], wout[:, columns], preferred_element_type=jnp.float32)
        part[:, :, columns] = product.astype(jnp.bfloat16).reshape(ntp, own_rows, tile)
        if (j + 1) % (tiles // strips) == 0:
            i = j // (tiles // strips)
            push(
                part.at[diagonal, :, strip_of(i)],
                rs_in.at[1, :, strip_of(i)],
                rs_recv.at[1 + i],
                me,
                mate,
            )
    push(part.at[mate], rs_in.at[2], rs_recv.at[0], me, mate)
    for j in range(strips):
        columns = slice(j * strip_width, (j + 1) * strip_width)
        arrived(rs_in.at[1, :, strip_of(j)], rs_recv.at[1 + j])
        part[across, :, columns] = (
            part[across, :, columns].astype(jnp.float32)
            + rs_in[1, :, columns].astype(jnp.float32)
        ).astype(jnp.bfloat16)
        push(
            part.at[across, :, strip_of(j)],
            rs_in.at[3, :, strip_of(j)],
            rs_recv.at[1 + strips + j],
            me,
            across,
        )
    loads[9].wait()
    loads[10].wait()
    arrived(rs_in.at[2], rs_recv.at[0])
    squares = jnp.zeros((own_rows, 1), jnp.float32)
    for j in range(strips):
        columns = slice(j * strip_width, (j + 1) * strip_width)
        early = (
            resid_ref[:, columns].astype(jnp.float32)
            + part[tp, :, columns].astype(jnp.float32)
            + rs_in[2, :, columns].astype(jnp.float32)
        )
        arrived(rs_in.at[3, :, strip_of(j)], rs_recv.at[1 + strips + j])
        total = early + rs_in[3, :, columns].astype(jnp.float32)
        squares = squares + jnp.sum(total * total, axis=-1, keepdims=True)
        state[:, columns] = total
    normed = (state[...] * lax.rsqrt(squares / width + norm_eps) * ngain_ref[...]).astype(
        jnp.bfloat16
    )
    mail[...] = (
        jnp.dot(placed_ref[...], normed, preferred_element_type=jnp.float32)
        .astype(jnp.bfloat16)
        .reshape(nsp, cap, width)
    )
    for d in LEAVING:
        to = peer(d)
        push(mail.at[to], inbox.at[tp, me], mail_recv.at[d], to, tp)
    inbox[tp, me] = mail[me]

    def group_of(groups, d):
        return next(g for g, group in enumerate(groups) if d in group)

    def spread(*pieces):
        for d in pieces:
            piece = inbox.at[tp, peer(d)]
            if d:
                arrived(piece, mail_recv.at[d])
            push(piece, piece, x_recv.at[d], me, across)
            push(piece, piece, mate_recv.at[group_of(O_GROUPS, d)], me, mate)

    def forward(*pieces):
        for d in pieces:
            piece = inbox.at[across, peer(d)]
            arrived(piece, x_recv.at[d])
            push(piece, piece, diagonal_recv.at[group_of(A_GROUPS, d)], me, mate)

    def settle_mate(g):
        arrived(inbox.at[mate, pl.ds(0, len(O_GROUPS[g]))], mate_recv.at[g])

    def settle_diagonal(g):
        arrived(inbox.at[diagonal, pl.ds(0, len(A_GROUPS[g]))], diagonal_recv.at[g])

    def runs_of(pieces):
        slots = sorted(ORDER.index(d) for d in pieces)
        starts = [slot for slot in slots if slot - 1 not in slots]
        ends = [slot + 1 for slot in slots if slot + 1 not in slots]
        return list(zip(starts, ends))

    def in_order(pieces):
        return sorted(pieces, key=ORDER.index)

    fine = 256

    def experts(parts, pieces, hooks):
        pieces = in_order(pieces)
        blocks = [(owner, peer(d)) for owner, _ in parts for d in pieces]
        live = len(blocks) * cap

        steps = wgate.shape[1] // fine
        for j in range(steps):
            columns = slice(j * fine, (j + 1) * fine)
            block = jnp.concatenate([inbox[owner, source] for owner, source in blocks], axis=0)
            gate = jnp.dot(block, wgate[:, columns], preferred_element_type=jnp.float32)
            up = jnp.dot(block, wup[:, columns], preferred_element_type=jnp.float32)
            hidden[:live, columns] = (gate / (1.0 + jnp.exp(-gate)) * up).astype(jnp.bfloat16)
            hooks(j - steps)

        for j in range(tiles):
            columns = slice(j * tile, (j + 1) * tile)
            product = jnp.dot(hidden[:live], wdown[:, columns], preferred_element_type=jnp.float32)
            product = product.reshape(len(parts), len(pieces), cap, tile)
            for i, (_, target) in enumerate(parts):
                done = 0
                for start, end in runs_of(pieces):
                    count = end - start
                    target[start:end, :, columns] = product[i, done : done + count].astype(
                        target.dtype
                    )
                    done += count
            hooks(j)

    def strip(ref, start, end, j):
        return ref.at[pl.ds(start, end - start), :, tile_of(j)]

    def hand(i, pieces, arrival, j):
        for start, end in runs_of(pieces):
            push(
                strip(pair_out.at[i], start, end, j),
                strip(pair_in.at[i], start, end, j),
                arrival,
                me,
                mate,
            )

    def take(i, pieces, arrival):
        arrived(pair_in.at[i, pl.ds(0, len(pieces))], arrival)

    def near_side(g, hooks):
        pieces = O_GROUPS[g]

        def each(j):
            if j >= 0:
                hand(0, pieces, near_recv.at[g], j)
            hooks(j)

        experts([(tp, keep.at[0]), (mate, pair_out.at[0])], pieces, each)

    def far_side(g, hooks):
        pieces = A_GROUPS[g]

        def each(j):
            if j >= 0:
                later_half = pieces == A_GROUPS[-1] and 2 * j >= tiles
                hand(1, pieces, far_recv.at[g + 1 if later_half else g], j)
            hooks(j)

        experts([(diagonal, pair_out.at[1]), (across, keep.at[1])], pieces, each)

    def cross(*order):
        for d in order:
            slot = ORDER.index(d)
            xsum[slot] = (keep[1, slot] + pair_in[1, slot].astype(jnp.float32)).astype(
                jnp.bfloat16
            )
            push(xsum.at[slot], xin.at[slot], rx_recv.at[slot], me, across)

    def half_columns(h):
        return pl.ds(h * (width // 2), width // 2)

    def half_arrival(d, h):
        return rx_recv.at[nsp + A_GROUPS[-1].index(d) if h else ORDER.index(d)]

    def take_half(h):
        last = A_GROUPS[-1]
        arrived(
            pair_in.at[1, pl.ds(0, len(last)), :, half_columns(h)],
            far_recv.at[len(A_GROUPS) - 1 + h],
        )

    def cross_half(h, *order):
        columns = slice(h * (width // 2), (h + 1) * (width // 2))
        for d in order:
            slot = ORDER.index(d)
            xsum[slot, :, columns] = (
                keep[1, slot, :, columns] + pair_in[1, slot, :, columns].astype(jnp.float32)
            ).astype(jnp.bfloat16)
            push(
                xsum.at[slot, :, half_columns(h)],
                xin.at[slot, :, half_columns(h)],
                half_arrival(d, h),
                me,
                across,
            )

    def finish_half(h, *pieces):
        columns = slice(h * (width // 2), (h + 1) * (width // 2))
        for d in pieces:
            slot = ORDER.index(d)
            arrived(xin.at[slot, :, half_columns(h)], half_arrival(d, h))
            outmail[slot, :, columns] = (
                keep[0, slot, :, columns]
                + pair_in[0, slot, :, columns].astype(jnp.float32)
                + xin[slot, :, columns].astype(jnp.float32)
            ).astype(jnp.bfloat16)
            push(
                outmail.at[slot, :, half_columns(h)],
                back.at[me, :, half_columns(h)],
                back_recv.at[0],
                peer(d),
                tp,
            )

    def finish(*pieces):
        for d in pieces:
            slot = ORDER.index(d)
            source = peer(d)
            arrived(xin.at[slot], rx_recv.at[slot])
            summed = (
                keep[0, slot]
                + pair_in[0, slot].astype(jnp.float32)
                + xin[slot].astype(jnp.float32)
            ).astype(jnp.bfloat16)
            if d:
                outmail[slot] = summed
                push(outmail.at[slot], back.at[me], back_recv.at[0], source, tp)
            else:
                back[me] = summed

    def plan(steps):
        table = {}
        for at, action in steps:
            table.setdefault(at, []).append(action)

        def run(j):
            for action in table.get(j, ()):
                action()

        return run

    def later(function, *given):
        return lambda: function(*given)

    def weights_here():
        for i in (12, 13, 14):
            loads[i].wait()

    simple = {
        "spread": spread,
        "forward": forward,
        "finish": finish,
        "take_half": take_half,
        "cross_half": cross_half,
        "finish_half": finish_half,
        "settle_mate": settle_mate,
        "settle_diagonal": settle_diagonal,
        "weights": weights_here,
        "cross": cross,
        "take_near": lambda g: take(0, O_GROUPS[g], near_recv.at[g]),
        "take_far": lambda g: take(1, A_GROUPS[g], far_recv.at[g]),
    }
    for kind, given, hooks in SCHEDULE:
        if kind in simple:
            simple[kind](*given)
            continue
        run = plan([(at, later(simple[what], *pieces)) for at, what, pieces in hooks])
        (near_side if kind == "near" else far_side)(*given, run)
    arrived(back.at[pl.ds(0, nsp - 1)], back_recv.at[0])
    for j in range(tiles):
        columns = slice(j * tile, (j + 1) * tile)
        returned = back[:, :, columns].reshape(nsp * cap, tile)
        result = state[:, columns]
        for i in range(picks.shape[0]):
            chosen = lax.dot_general(
                picks[i], returned, (((0,), (0,)), ((), ())), preferred_element_type=jnp.float32
            )
            result = result + wcol[i, :, 0:1] * chosen
        out_ref[:, columns] = result.astype(out_ref.dtype)
    assert sum(sent) == math.prod(gone.shape)
    pltpu.make_async_remote_copy(
        src_ref=gone,
        dst_ref=gone,
        send_sem=send_sem.at[0],
        recv_sem=back_recv.at[0],
        device_id=(twin, tp),
        device_id_type=MESH,
    ).wait_send()


def pinned(array):
    return pltpu.with_memory_space_constraint(jnp.asarray(array), pltpu.MemorySpace.HBM)


def grid_tables(nsp, rows):
    count = HEAD_SIZE // 4
    inverse = theta_base ** (-np.arange(count, dtype=np.float64) * 2.0 / (HEAD_SIZE // 2))
    inverse = np.tile(inverse.astype(np.float32), 4)[None, :]

    def both(amount):
        angles = np.arange(amount, dtype=np.float32)[:, None] * inverse
        pair = [np.cos(angles), np.sin(angles)]
        return np.concatenate(pair, axis=1).astype(np.float32)

    lines = rows // GRID_W
    return both(nsp * lines).reshape(nsp, lines, 2 * HEAD_SIZE), both(GRID_W)


def sent_rows(nsp, ntp, rows, own_rows, cap, width):
    attention = 2 * (nsp - 1) * rows * HEAD_SIZE // width
    return attention + (ntp - 1) * own_rows + (2 * (nsp - 1) + 6 * nsp) * cap


def on_device_fused(
    queries,
    keys,
    values,
    query_gain,
    key_norm_gain,
    out_weight,
    residual,
    norm_gain,
    expert_gate,
    expert_up,
    expert_down,
    routes,
    route_weight,
):
    nsp = lax.axis_size("sp")
    ntp = lax.axis_size("tp")
    rows = queries.shape[0]
    heads = queries.shape[1] // HEAD_SIZE
    own_rows, width = residual.shape
    top = routes.shape[1]
    cap = 2 * max(1, top * rows // (ntp * nsp))
    hidden_units = expert_gate.shape[2]
    by_row, by_column = grid_tables(nsp, rows)
    vmem = pl.BlockSpec(memory_space=pltpu.VMEM)
    hbm = pl.BlockSpec(memory_space=pltpu.MemorySpace.HBM)
    half, full = jnp.bfloat16, jnp.float32
    dma = pltpu.SemaphoreType.DMA
    return pl.pallas_call(
        functools.partial(layer_kernel, (nsp, ntp, heads, cap, rows, own_rows)),
        out_shape=jax.ShapeDtypeStruct((own_rows, width), half),
        in_specs=[hbm] * 15,
        out_specs=vmem,
        scratch_shapes=[
            pltpu.VMEM(by_row.shape[1:], full),
            pltpu.VMEM(by_column.shape, full),
            pltpu.VMEM(keys.shape, half),
            pltpu.VMEM((1, HEAD_SIZE), full),
            pltpu.VMEM(queries.shape, half),
            pltpu.VMEM((1, HEAD_SIZE), full),
            pltpu.VMEM((top, own_rows), jnp.int32),
            pltpu.VMEM((top, own_rows), full),
            pltpu.VMEM((own_rows, width), half),
            pltpu.VMEM((1, width), full),
            pltpu.VMEM((top, nsp * cap, own_rows), half),
            pltpu.VMEM((nsp * cap, own_rows), half),
            pltpu.VMEM((top, own_rows, HEAD_SIZE), full),
            pltpu.VMEM(out_weight.shape, half),
            pltpu.VMEM(expert_gate.shape[1:], half),
            pltpu.VMEM(expert_up.shape[1:], half),
            pltpu.VMEM(expert_down.shape[1:], half),
            pltpu.VMEM((nsp, rows, HEAD_SIZE), half),
            pltpu.VMEM((nsp, rows, HEAD_SIZE), half),
            pltpu.VMEM((heads, rows, nsp * rows), half),
            pltpu.VMEM((heads, rows, HEAD_SIZE), full),
            pltpu.VMEM(queries.shape, half),
            pltpu.VMEM((ntp, own_rows, width), half),
            pltpu.VMEM((ntp, own_rows, width), half),
            pltpu.VMEM((own_rows, width), full),
            pltpu.VMEM((nsp, cap, width), half),
            pltpu.VMEM((ntp, nsp, cap, width), half),
            pltpu.VMEM((2 * LARGEST * cap, hidden_units), half),
            pltpu.VMEM((2, nsp, cap, width), full),
            pltpu.VMEM((2, nsp, cap, width), half),
            pltpu.VMEM((2, nsp, cap, width), half),
            pltpu.VMEM((nsp, cap, width), half),
            pltpu.VMEM((nsp, cap, width), half),
            pltpu.VMEM((nsp, cap, width), half),
            pltpu.VMEM((nsp, cap, width), half),
            dma((15,)),
            pltpu.VMEM((sent_rows(nsp, ntp, rows, own_rows, cap, width), width), half),
            dma((1,)),
            dma((3,)),
            dma((3,)),
            dma((5,)),
            dma((nsp,)),
            dma((len(O_GROUPS),)),
            dma((nsp,)),
            dma((len(A_GROUPS),)),
            dma((len(O_GROUPS),)),
            dma((len(A_GROUPS) + 1,)),
            dma((nsp + len(A_GROUPS[-1]),)),
            dma((1,)),
        ],
        compiler_params=pltpu.CompilerParams(
            collective_id=0, has_side_effects=True, vmem_limit_bytes=40_000_000
        ),
    )(
        *map(
            pinned,
            (
                by_row,
                by_column,
                keys,
                key_norm_gain[None, :],
                values,
                queries,
                query_gain[None, :],
                out_weight,
                routes.T,
                route_weight.T,
                residual,
                norm_gain[None, :],
                expert_gate,
                expert_up,
                expert_down,
            ),
        )
    )


def fits_fused(mesh):
    return mesh.shape["tp"] == 4 and mesh.shape["sp"] == 8


def solution(mesh):
    body = on_device_fused if fits_fused(mesh) else on_device
    placed = (
        P("sp", "tp"),
        P("sp", "tp"),
        P("sp", "tp"),
        P(),
        P(),
        P("tp", None),
        P(("sp", "tp"), None),
        P(),
        P("sp", None, "tp"),
        P("sp", None, "tp"),
        P("sp", "tp", None),
        P(("sp", "tp"), None),
        P(("sp", "tp"), None),
    )
    return jax.shard_map(
        body, mesh=mesh, in_specs=placed, out_specs=P(("sp", "tp"), None), check_vma=False
    )
```
